128 devices in a mesh: sp: 16 (over z, y), dp: 8 (over x, core).
Axes of the slice: x: 4, y: 4, z: 4, core: 2. Of those that a mesh axis runs over, the one named last changes fastest.
Arguments:
- stream: bfloat16 [8, 2048, 2048], P('dp', 'sp'), may hold values from -6 to 6
- queries: bfloat16 [8, 2048, 1024], P('dp', 'sp'), may hold values from -6 to 6
- keys_in: bfloat16 [8, 2048, 1024], P('dp', 'sp'), may hold values from -6 to 6
- values_in: bfloat16 [8, 2048, 1024], P('dp', 'sp'), may hold values from -6 to 6
- key_shift: bfloat16 [8, 2048, 16], P('dp', 'sp'), may hold values from -8 to 16
- head_shift: float32 [16], replicated, may hold values from -16 to 0
- mix_gain: float32 [1024], replicated, may hold values from 0.1 to 1.9
- out_weight: bfloat16 [1024, 2048], replicated, may hold values from -0.1875 to 0.1875
- post_gain: float32 [2048], replicated, may hold values from 0.1 to 1.9
- route: int32 [8, 2048, 2], P('dp', 'sp'), may hold values from 0 to 127, as said below
- route_weight: float32 [8, 2048, 2], P('dp', 'sp'), may hold values from 0.25 to 1
- w_gate: bfloat16 [128, 2048, 1024], P(('sp', 'dp')), may hold values from -0.125 to 0.125
- w_up: bfloat16 [128, 2048, 1024], P(('sp', 'dp')), may hold values from -0.125 to 0.125
- w_down: bfloat16 [128, 1024, 2048], P(('sp', 'dp')), may hold values from -0.1875 to 0.1875
Outputs:
- result: bfloat16 [8, 2048, 2048], P('dp', 'sp')
The draws below stay inside these ranges and needn't reach their ends.
Inputs may be any that keep to these rules, and one draw needn't show every extreme that they name: `route`: each token names two different experts of one group (the group of expert e is e // 32). Of the 128 tokens of one device, each expert is named by at most 4; in every draw the 32 experts of one group are each named by exactly 4 tokens of every device.
All inputs are finite; a program needn't handle non-finite values.
Results may differ from the reference program's by a relative error of at most 0.0085.
Values may be sent and summed in bfloat16 or wider, within the bound.
A program may use at most 128 MiB of HBM per device.

```python
import math
import jax
import jax.numpy as jnp
from jax import lax

D = 2048
HEADS = 16
HD = 64
F = 1024
GROUPS = 4
TOK_DEV = 128
SEQUENCE_LENGTH = 2048
SEQUENCE_COUNT = 8
EXPERTS = 128
EPG = 32
CAP = 4
N_SP = 16
N_DP = 8


def head_rates(key):
    base = jax.random.fold_in(key, 11)
    share = jax.random.uniform(base, (HEADS,), jnp.float32, 0.4, 1.4)
    return -share * math.log(SEQUENCE_LENGTH)


def draw_head_shift(key, part):
    return head_rates(key)


def draw_key_shift(key, part):
    decay_rates = head_rates(key)
    random_jitter = jnp.clip(0.7 * jax.random.normal(jax.random.fold_in(key, 12), (SEQUENCE_COUNT, SEQUENCE_LENGTH // TOK_DEV, TOK_DEV, HEADS), jnp.float32), -3.0, 3.0)
    offset = jax.random.uniform(jax.random.fold_in(key, 13), (SEQUENCE_COUNT, SEQUENCE_LENGTH // TOK_DEV, 1, HEADS), jnp.float32, -0.7, 0.7)
    random_jitter = (random_jitter + offset).reshape(SEQUENCE_COUNT, SEQUENCE_LENGTH, HEADS)
    sudden_spike = jax.random.randint(jax.random.fold_in(key, 14), (SEQUENCE_COUNT, SEQUENCE_LENGTH, 1), 0, max(SEQUENCE_LENGTH // 4, 2)) == 0
    value_entry = jnp.where(sudden_spike, -decay_rates[None, None, :] - 0.7, random_jitter)
    return value_entry.astype(jnp.bfloat16)


def draw_route(key, part):
    nblocks = SEQUENCE_COUNT * (SEQUENCE_LENGTH // TOK_DEV)
    half = TOK_DEV // 2
    hot = jax.random.randint(jax.random.fold_in(key, 21), (), 0, GROUPS)
    cuts = jnp.sort(jax.random.randint(jax.random.fold_in(key, 22), (nblocks, GROUPS - 2), 0, half + 1), axis=1)
    bounds = jnp.concatenate([jnp.zeros((nblocks, 1), jnp.int32), cuts, jnp.full((nblocks, 1), half, jnp.int32)], axis=1)
    others = bounds[:, 1:] - bounds[:, :-1]
    sizes = jnp.concatenate([jnp.full((nblocks, 1), half, jnp.int32), others], axis=1)
    ends = jnp.cumsum(sizes, axis=1)
    starts = ends - sizes
    position = jnp.arange(TOK_DEV, dtype=jnp.int32)
    section = jnp.sum((position[None, :, None] >= ends[:, None, :]).astype(jnp.int32), axis=2)
    within = position[None, :] - jnp.take_along_axis(starts, section, axis=1)
    group = (hot + section) % GROUPS
    per_row = EPG // 2
    row_idx = within // per_row
    col_idx = within % per_row
    scores = jax.random.randint(jax.random.fold_in(key, 23), (nblocks, GROUPS, CAP, EPG), 0, 2 ** 20) * EPG + jnp.arange(EPG, dtype=jnp.int32)
    perm = jnp.argsort(scores, axis=-1, stable=True).astype(jnp.int32).reshape(nblocks, GROUPS * CAP * EPG)
    flat_idx = (section * CAP + row_idx) * EPG + 2 * col_idx
    first = jnp.take_along_axis(perm, flat_idx, axis=1) + group * EPG
    second = jnp.take_along_axis(perm, flat_idx + 1, axis=1) + group * EPG
    pairs = jnp.stack([first, second], axis=2)
    tscore = jax.random.randint(jax.random.fold_in(key, 24), (nblocks, TOK_DEV), 0, 2 ** 20) * TOK_DEV + position[None, :]
    placement = jnp.argsort(tscore, axis=1, stable=True).astype(jnp.int32)
    shuffled = jnp.take_along_axis(pairs, placement[:, :, None], axis=1)
    return shuffled.reshape(SEQUENCE_COUNT, SEQUENCE_LENGTH, 2).astype(jnp.int32)


def steps_of(rng, dims, cuts, low, high):
    loudness, own = 1.0, jax.random.fold_in(rng, 6)
    for axis_at, blocks in cuts:
        heights = jnp.exp(jax.random.uniform(jax.random.fold_in(own, axis_at), (blocks,), jnp.float32, low / len(cuts), high / len(cuts)))
        loudness = loudness * jnp.repeat(heights, dims[axis_at] // blocks).reshape([-1 if axis == axis_at else 1 for axis in range(len(dims))])
    return loudness


def noise(key, dims, scale, most, cuts=(), kind=jnp.bfloat16):
    drawn = scale * jax.random.normal(key, dims, jnp.float32)
    if cuts:
        drawn = drawn * steps_of(key, dims, cuts, -0.22, 0.18)
    return jnp.clip(drawn, -most, most).astype(kind)


def setup_inputs(seed: int = 0) -> dict:
    arg_keys = jax.random.split(jax.random.key(seed), 15)
    stream = noise(arg_keys[0], (SEQUENCE_COUNT, SEQUENCE_LENGTH, D), 1.0, 6.0, ((0, 8), (1, 16)))
    queries = noise(arg_keys[1], (SEQUENCE_COUNT, SEQUENCE_LENGTH, HEADS * HD), 1.0, 6.0, ((0, 8), (1, 16)))
    keys_in = noise(arg_keys[2], (SEQUENCE_COUNT, SEQUENCE_LENGTH, HEADS * HD), 1.0, 6.0, ((0, 8), (1, 16)))
    values_in = noise(arg_keys[3], (SEQUENCE_COUNT, SEQUENCE_LENGTH, HEADS * HD), 1.0, 6.0, ((0, 8), (1, 16)))
    key_shift = draw_key_shift(jax.random.fold_in(arg_keys[14], 71), 0)
    head_shift = draw_head_shift(jax.random.fold_in(arg_keys[14], 71), 0)
    mix_gain = jnp.clip(1.0 + 0.18 * jax.random.normal(arg_keys[6], (HEADS * HD,), jnp.float32), 0.1, 1.9)
    out_weight = noise(arg_keys[7], (HEADS * HD, D), (HEADS * HD) ** -0.5, 0.1875)
    post_gain = jnp.clip(1.0 + 0.18 * jax.random.normal(arg_keys[8], (D,), jnp.float32), 0.1, 1.9)
    route = draw_route(jax.random.fold_in(arg_keys[14], 71), 0)
    route_weight = jnp.clip(jnp.exp(math.log(1.0) - 1.3862944 * jax.random.uniform(arg_keys[10], (SEQUENCE_COUNT, SEQUENCE_LENGTH, 2), jnp.float32) ** steps_of(arg_keys[10], (SEQUENCE_COUNT, SEQUENCE_LENGTH, 2), ((0, 8), (1, 16)), -0.2, 0.2)), 0.25, 1.0)
    w_gate = noise(arg_keys[11], (EXPERTS, D, F), D ** -0.5, 0.125, ((0, 128),))
    w_up = noise(arg_keys[12], (EXPERTS, D, F), D ** -0.5, 0.125, ((0, 128),))
    w_down = noise(arg_keys[13], (EXPERTS, F, D), F ** -0.5, 0.1875, ((0, 128),))
    return dict(stream=stream, queries=queries, keys_in=keys_in, values_in=values_in, key_shift=key_shift, head_shift=head_shift, mix_gain=mix_gain, out_weight=out_weight, post_gain=post_gain, route=route, route_weight=route_weight, w_gate=w_gate, w_up=w_up, w_down=w_down)


norm_eps = 1e-05

def block_total(length):
    blocks = 1
    while blocks * 2 <= min(8, length // 512):
        blocks = blocks * 2
    return blocks

def stick_head(queries_head, keys_head, values_head, offsets):
    length = queries_head.shape[0]
    blocks = block_total(length)
    width = length // blocks
    scale = 1.0 / math.sqrt(HD)
    pieces = []
    for block_idx in range(blocks):
        begin = block_idx * width
        finish = begin + width
        logits = jnp.dot(queries_head[begin:finish].astype(jnp.float32), keys_head[:finish].astype(jnp.float32).T, precision=lax.Precision.HIGHEST, preferred_element_type=jnp.float32) * scale
        logits = logits + offsets[None, :finish]
        rows_pos = begin + jnp.arange(width, dtype=jnp.int32)
        cols_pos = jnp.arange(finish, dtype=jnp.int32)
        causal = cols_pos[None, :] < rows_pos[:, None]
        breaks = jnp.where(causal, jax.nn.log_sigmoid(-logits), 0.0)
        suffix = lax.cumsum(breaks, axis=1, reverse=True) - breaks
        weights = jnp.where(causal, jnp.exp(jax.nn.log_sigmoid(logits) + suffix), 0.0).astype(jnp.bfloat16)
        pieces.append(jnp.dot(weights.astype(jnp.float32), values_head[:finish].astype(jnp.float32), precision=lax.Precision.HIGHEST, preferred_element_type=jnp.float32))
    return jnp.concatenate(pieces, axis=0)

def reference(stream, queries, keys_in, values_in, key_shift, head_shift, mix_gain, out_weight, post_gain, route, route_weight, w_gate, w_up, w_down):

    def by_head(array):
        return array.reshape(SEQUENCE_COUNT, SEQUENCE_LENGTH, HEADS, HD).transpose(0, 2, 1, 3).reshape(SEQUENCE_COUNT * HEADS, SEQUENCE_LENGTH, HD)
    offsets = key_shift.astype(jnp.float32).transpose(0, 2, 1) + head_shift[None, :, None]
    offsets = offsets.reshape(SEQUENCE_COUNT * HEADS, SEQUENCE_LENGTH)

    def one_head(items):
        return stick_head(items[0], items[1], items[2], items[3]).astype(jnp.bfloat16)
    attended = lax.map(one_head, (by_head(queries), by_head(keys_in), by_head(values_in), offsets))
    attended = attended.reshape(SEQUENCE_COUNT, HEADS, SEQUENCE_LENGTH, HD).transpose(0, 2, 1, 3).reshape(SEQUENCE_COUNT * SEQUENCE_LENGTH, HEADS * HD)
    att32 = attended.astype(jnp.float32)
    normed = (att32 * lax.rsqrt(lax.optimization_barrier(jnp.mean(att32 * att32, axis=1, keepdims=True)) + norm_eps) * mix_gain).astype(jnp.bfloat16)
    mixed = jnp.dot(normed.astype(jnp.float32), out_weight.astype(jnp.float32), precision=lax.Precision.HIGHEST, preferred_element_type=jnp.float32)
    summed = stream.reshape(SEQUENCE_COUNT * SEQUENCE_LENGTH, D).astype(jnp.float32) + mixed
    hidden = (summed * lax.rsqrt(lax.optimization_barrier(jnp.mean(summed * summed, axis=1, keepdims=True)) + norm_eps) * post_gain).astype(jnp.bfloat16)
    total = SEQUENCE_COUNT * SEQUENCE_LENGTH
    expert_ids = route.reshape(total * 2).astype(jnp.int32)
    weights_flat = route_weight.reshape(total * 2)
    order = jnp.argsort(expert_ids, stable=True).astype(jnp.int32)
    tok_sorted = order // 2
    weight_sorted = weights_flat[order]
    counts = lax.optimization_barrier(jnp.sum((expert_ids[:, None] == jnp.arange(EXPERTS, dtype=jnp.int32)[None, :]).astype(jnp.int32), axis=0))
    starts = (jnp.cumsum(counts) - counts).astype(jnp.int32)
    most_rows = N_SP * N_DP * CAP
    tok_padded = jnp.concatenate([tok_sorted, jnp.zeros((most_rows,), jnp.int32)])
    weight_padded = jnp.concatenate([weight_sorted, jnp.zeros((most_rows,), jnp.float32)])

    def one_expert(carry, expert):
        index_rows = lax.dynamic_slice(tok_padded, (starts[expert],), (most_rows,))
        weight_rows = lax.dynamic_slice(weight_padded, (starts[expert],), (most_rows,))
        valid = jnp.arange(most_rows, dtype=jnp.int32) < counts[expert]
        rows = hidden[index_rows].astype(jnp.float32)
        gate = jnp.dot(rows, w_gate[expert].astype(jnp.float32), precision=lax.Precision.HIGHEST, preferred_element_type=jnp.float32)
        upper = jnp.dot(rows, w_up[expert].astype(jnp.float32), precision=lax.Precision.HIGHEST, preferred_element_type=jnp.float32)
        inner = (jax.nn.silu(gate) * upper).astype(jnp.bfloat16)
        output = jnp.dot(inner.astype(jnp.float32), w_down[expert].astype(jnp.float32), precision=lax.Precision.HIGHEST, preferred_element_type=jnp.float32).astype(jnp.bfloat16)
        scaled_values = jnp.where(valid[:, None], weight_rows[:, None] * output.astype(jnp.float32), 0.0)
        return (carry.at[index_rows].add(scaled_values), None)
    moe_sum, _ = lax.scan(one_expert, jnp.zeros((total, D), jnp.float32), jnp.arange(EXPERTS, dtype=jnp.int32))
    result = (hidden.astype(jnp.float32) + moe_sum).astype(jnp.bfloat16)
    return result.reshape(SEQUENCE_COUNT, SEQUENCE_LENGTH, D)
```

```python
import jax
import jax.numpy as jnp
from jax import lax
from jax.sharding import PartitionSpec as P
from jax.experimental import pallas as pl
from jax.experimental.pallas import tpu as pltpu

GROUPS = 4
EXP_DEV = 1
SP = "sp"
SP_DP = ("sp", "dp")


norm_eps = 1e-05


LOG2E = 1.4426950408889634
KB = 256
QB = 256
NT = (((1,), (1,)), ((), ()))
BF16 = jnp.bfloat16
F32 = jnp.float32


def picker(rows, cols, fn):
    r = lax.broadcasted_iota(jnp.int32, (rows, cols), 0)
    c = lax.broadcasted_iota(jnp.int32, (rows, cols), 1)
    return jnp.where(fn(r, c), 1.0, 0.0).astype(BF16)


def f32dot(a, b):
    return jnp.dot(a, b, preferred_element_type=F32)


def half_pickers():
    low_low = picker(128, 128, lambda r, c: (r == c) & (c < 64))
    low_high = picker(128, 128, lambda r, c: r == c - 64)
    high_low = picker(128, 128, lambda r, c: r == c + 64)
    high_high = picker(128, 128, lambda r, c: (r == c) & (c >= 64))
    return (low_low, low_high), (high_low, high_high)


def mixer_kernel(
    q_ref, k_ref, v_ref, shift_ref, head_shift_ref, stream_ref, mix_ref, w_ref, post_ref,
    hidden_ref,
    sendbuf, recvbuf, attsend, attrecv, qs, kk, vv, off, w_vmem, normed,
    send_sem, recv_sem, asend_sem, arecv_sem, w_sem,
):
    me = lax.axis_index("sp")
    barrier = pltpu.get_barrier_semaphore()
    for d in range(1, 16):
        pl.semaphore_signal(
            barrier, inc=1, device_id={"sp": lax.rem(me + d, 16)}, device_id_type=pl.DeviceIdType.MESH
        )
    w_copy = pltpu.make_async_copy(w_ref, w_vmem, w_sem)
    w_copy.start()

    pickers = half_pickers()
    shifts = lax.dot_general(
        picker(16, 16, lambda r, c: r == c), shift_ref[...], NT, preferred_element_type=F32
    )
    for h in range(16):
        tile = slice((h // 2) * 128, (h // 2 + 1) * 128)
        first, second = pickers[h % 2]
        sendbuf[h, 0:128, :] = (f32dot(q_ref[:, tile], first) + f32dot(k_ref[:, tile], second)).astype(BF16)
        sendbuf[h, 128:192, :] = (
            f32dot(v_ref[0:64, tile], first) + f32dot(v_ref[64:128, tile], second)
        ).astype(BF16)
        sendbuf[h, 192:208, :] = jnp.broadcast_to(shifts[h:h + 1, :], (16, 128)).astype(BF16)

    pl.semaphore_wait(barrier, 15)

    def outgoing(d):
        to = lax.rem(me + d, 16)
        return pltpu.make_async_remote_copy(
            src_ref=sendbuf.at[to],
            dst_ref=recvbuf.at[me],
            send_sem=send_sem.at[d],
            recv_sem=recv_sem.at[d],
            device_id={"sp": to},
            device_id_type=pl.DeviceIdType.MESH,
        )

    for d in range(1, 16):
        outgoing(d).start()
    recvbuf[me] = sendbuf[me]
    for d in range(1, 16):
        outgoing(d).wait()

    both_low = picker(128, 128, lambda r, c: r == c % 64)
    both_high = picker(128, 128, lambda r, c: r == c % 64 + 64)
    lane = lax.broadcasted_iota(jnp.int32, (128, 128), 1)
    hs = head_shift_ref[0]
    for j in range(16):
        rows = slice(j * 128, (j + 1) * 128)
        qk = recvbuf[j, 0:128, :]
        q2 = f32dot(qk, both_low) * (LOG2E / 8.0)
        hi = q2.astype(BF16).astype(F32)
        qs[rows, :] = jnp.where(lane < 64, hi, q2 - hi).astype(BF16)
        kk[rows, :] = f32dot(qk, both_high).astype(BF16)
        vm = recvbuf[j, 128:192, :]
        vv[j * 128:j * 128 + 64, :] = f32dot(vm, both_low).astype(BF16)
        vv[j * 128 + 64:j * 128 + 128, :] = f32dot(vm, both_high).astype(BF16)
        off[0:1, rows] = (recvbuf[j, 192:208, :].astype(F32)[0:1] + hs) * LOG2E

    tri = picker(KB, KB, lambda r, c: r >= c)
    lane64 = lax.broadcasted_iota(jnp.int32, (64, 128), 1) < 64

    def reply(j):
        return pltpu.make_async_remote_copy(
            src_ref=attsend.at[j],
            dst_ref=attrecv.at[me],
            send_sem=asend_sem.at[j],
            recv_sem=arecv_sem.at[me],
            device_id={"sp": j},
            device_id_type=pl.DeviceIdType.MESH,
        )

    for qi in range(2048 // QB):
        r0 = qi * QB
        carry = jnp.zeros((QB, 1), F32)
        acc = jnp.zeros((QB, 128), F32)
        for ki in range(qi, -1, -1):
            k0 = ki * KB
            z = lax.dot_general(qs[r0:r0 + QB, :], kk[k0:k0 + KB, :], NT, preferred_element_type=F32)
            z = z + off[0:1, k0:k0 + KB]
            sp = jnp.maximum(z, jnp.log2(1.0 + jnp.exp2(jnp.minimum(z, 100.0))))
            if ki == qi:
                r = lax.broadcasted_iota(jnp.int32, (QB, KB), 0)
                c = lax.broadcasted_iota(jnp.int32, (QB, KB), 1)
                sp = jnp.where(c < r, sp, 0.0)
            hi = sp.astype(BF16)
            lo = (sp - hi.astype(F32)).astype(BF16)
            s = f32dot(hi, tri) + f32dot(lo, tri)
            w = jnp.exp2(z - (s + carry))
            if ki == qi:
                w = jnp.where(c < r, w, 0.0)
            acc = acc + f32dot(w.astype(BF16), vv[k0:k0 + KB, :])
            carry = carry + s[:, 0:1]
        for part in range(QB // 128):
            j = r0 // 128 + part
            at = part * 128
            attsend[j] = jnp.where(lane64, acc[at:at + 64], acc[at + 64:at + 128]).astype(BF16)

            @pl.when(me != j)
            def _():
                reply(j).start()

            @pl.when(me == j)
            def _():
                attrecv[j] = attsend[j]

    for j in range(16):
        @pl.when(me != j)
        def _():
            reply(j).wait_send()
            pltpu.make_async_remote_copy(
                src_ref=attsend.at[j],
                dst_ref=attrecv.at[j],
                send_sem=asend_sem.at[j],
                recv_sem=arecv_sem.at[j],
                device_id={"sp": j},
                device_id_type=pl.DeviceIdType.MESH,
            ).wait_recv()

    (low_low, low_high), (high_low, high_high) = pickers
    squares = jnp.zeros((128, 1), F32)
    tiles = []
    for p in range(8):
        even, odd = attrecv[2 * p], attrecv[2 * p + 1]
        low = f32dot(even, low_low) + f32dot(odd, low_high)
        high = f32dot(even, high_low) + f32dot(odd, high_high)
        tile = jnp.concatenate([low, high], axis=0)
        squares = squares + jnp.sum(tile * tile, axis=1, keepdims=True)
        tiles.append(tile)
    inv = lax.rsqrt(squares * (1.0 / 1024.0) + norm_eps)
    for p in range(8):
        cols = slice(p * 128, (p + 1) * 128)
        normed[:, cols] = (tiles[p] * inv * mix_ref[:, cols]).astype(BF16)
    w_copy.wait()
    totals = jnp.zeros((128, 1), F32)
    sums = []
    for n in range(8):
        cols = slice(n * 256, (n + 1) * 256)
        summed = stream_ref[:, cols].astype(F32) + f32dot(normed[...], w_vmem[:, cols])
        totals = totals + jnp.sum(summed * summed, axis=1, keepdims=True)
        sums.append(summed)
    inv = lax.rsqrt(totals * (1.0 / 2048.0) + norm_eps)
    for n in range(8):
        cols = slice(n * 256, (n + 1) * 256)
        hidden_ref[:, cols] = (sums[n] * inv * post_ref[:, cols]).astype(BF16)


def mixer(q, k, v, shift, head_shift, stream, mix_gain, out_weight, post_gain):
    vmem = pl.BlockSpec(memory_space=pltpu.VMEM)
    return pl.pallas_call(
        mixer_kernel,
        out_shape=jax.ShapeDtypeStruct((128, 2048), BF16),
        in_specs=[vmem] * 4 + [pl.BlockSpec(memory_space=pltpu.SMEM)] + [vmem] * 2
        + [pl.BlockSpec(memory_space=pl.ANY), vmem],
        out_specs=vmem,
        scratch_shapes=[
            pltpu.VMEM((16, 208, 128), BF16),
            pltpu.VMEM((16, 208, 128), BF16),
            pltpu.VMEM((16, 64, 128), BF16),
            pltpu.VMEM((16, 64, 128), BF16),
            pltpu.VMEM((2048, 128), BF16),
            pltpu.VMEM((2048, 128), BF16),
            pltpu.VMEM((2048, 128), BF16),
            pltpu.VMEM((8, 2048), F32),
            pltpu.VMEM((1024, 2048), BF16),
            pltpu.VMEM((128, 1024), BF16),
            pltpu.SemaphoreType.DMA((16,)),
            pltpu.SemaphoreType.DMA((16,)),
            pltpu.SemaphoreType.DMA((16,)),
            pltpu.SemaphoreType.DMA((16,)),
            pltpu.SemaphoreType.DMA,
        ],
        compiler_params=pltpu.CompilerParams(
            collective_id=1, has_side_effects=True, vmem_limit_bytes=56 * 2**20
        ),
    )(q, k, v, shift, head_shift, stream, mix_gain, out_weight, post_gain)


def split_up(x, dim, length):
    lengths = x.shape
    pieces = x.reshape(*lengths[:dim], length, lengths[dim] // length, *lengths[dim + 1 :])
    return jnp.moveaxis(pieces, dim, 0)


def in_order(pieces, dim):
    lengths = list(pieces.shape[1:])
    lengths[dim] *= pieces.shape[0]
    return jnp.moveaxis(pieces, 0, dim).reshape(lengths)


def joined_exchange(x, axis, axes, splits, concats):
    sizes = [lax.axis_size(a) for a in axes]
    pieces = split_up(x, splits[0], sizes[0])
    pieces = jnp.moveaxis(split_up(pieces, splits[1] + 1, sizes[1]), 0, 1)
    inside = pieces.shape[2:]
    pieces = pieces.reshape(-1, *inside)
    pieces = lax.all_to_all(pieces, axis, split_axis=0, concat_axis=0, tiled=True)
    pieces = in_order(pieces.reshape(*sizes, *inside), concats[0] + 1)
    return in_order(pieces, concats[1])


def on_device(
    stream,
    queries,
    keys_in,
    values_in,
    key_shift,
    head_shift,
    mix_gain,
    out_weight,
    post_gain,
    route,
    route_weight,
    w_gate,
    w_up,
    w_down,
):
    tokens = stream.shape[1]
    width = stream.shape[2]
    own_shift = lax.dynamic_slice_in_dim(head_shift, lax.axis_index(SP), 1)
    hidden = mixer(
        queries[0], keys_in[0], values_in[0], key_shift[0], own_shift, stream[0],
        mix_gain[None], out_weight, post_gain[None],
    )
    size_sp = lax.axis_size(SP)
    size_dp = lax.axis_size("dp")
    n_expert = EXP_DEV * size_sp * size_dp
    per_group = n_expert // GROUPS
    capacity = tokens // per_group
    expert_ids = route[0].reshape(tokens * 2)
    onehot = (expert_ids[:, None] == jnp.arange(n_expert, dtype=jnp.int32)[None, :]).astype(
        jnp.int32
    )
    ranks = jnp.sum((jnp.cumsum(onehot, axis=0) - onehot) * onehot, axis=1)
    dest = expert_ids * capacity + ranks
    rows = jnp.repeat(hidden, 2, axis=0)
    buffer = jnp.zeros((n_expert * capacity, width), jnp.bfloat16).at[dest].set(rows)
    sendable = buffer.reshape(size_sp, size_dp, EXP_DEV * capacity, width)
    received = joined_exchange(sendable, SP_DP, (SP, "dp"), (0, 1), (0, 1))
    expert_received = received.reshape(size_sp * size_dp, EXP_DEV, capacity, width)
    gate = jnp.einsum("sxcd,xdf->sxcf", expert_received, w_gate, preferred_element_type=jnp.float32)
    upper = jnp.einsum("sxcd,xdf->sxcf", expert_received, w_up, preferred_element_type=jnp.float32)
    inner = (jax.nn.silu(gate) * upper).astype(jnp.bfloat16)
    reply_result = jnp.einsum(
        "sxcf,xfd->sxcd", inner, w_down, preferred_element_type=jnp.float32
    ).astype(jnp.bfloat16)
    reply_result = reply_result.reshape(size_sp, size_dp, EXP_DEV * capacity, width)
    returned = joined_exchange(reply_result, SP_DP, (SP, "dp"), (0, 1), (0, 1))
    returned = returned.reshape(n_expert * capacity, width)
    picked = returned[dest].astype(jnp.float32).reshape(tokens, 2, width)
    moe_sum = jnp.sum(picked * route_weight[0][:, :, None], axis=1)
    result = (hidden.astype(jnp.float32) + moe_sum).astype(jnp.bfloat16)
    return result[None]


def solution(mesh):
    placed = (
        P("dp", SP, None),
        P("dp", SP, None),
        P("dp", SP, None),
        P("dp", SP, None),
        P("dp", SP, None),
        P(),
        P(),
        P(),
        P(),
        P("dp", SP, None),
        P("dp", SP, None),
        P(SP_DP, None, None),
        P(SP_DP, None, None),
        P(SP_DP, None, None),
    )
    return jax.shard_map(
        on_device, mesh=mesh, in_specs=placed, out_specs=P("dp", SP, None), check_vma=False
    )
```

```python
import jax
import jax.numpy as jnp
from jax import lax
from jax.sharding import PartitionSpec as P
from jax.experimental import pallas as pl
from jax.experimental.pallas import tpu as pltpu

SP = "sp"
SP_DP = ("sp", "dp")
norm_eps = 1e-05
LOG2E = 1.4426950408889634
KB = 256
QB = 256
NT = (((1,), (1,)), ((), ()))
BF16 = jnp.bfloat16
F32 = jnp.float32


def picker(rows, cols, fn):
    r = lax.broadcasted_iota(jnp.int32, (rows, cols), 0)
    c = lax.broadcasted_iota(jnp.int32, (rows, cols), 1)
    return jnp.where(fn(r, c), 1.0, 0.0).astype(BF16)


def f32dot(a, b):
    return jnp.dot(a, b, preferred_element_type=F32)


def half_pickers():
    low_low = picker(128, 128, lambda r, c: (r == c) & (c < 64))
    low_high = picker(128, 128, lambda r, c: r == c - 64)
    high_low = picker(128, 128, lambda r, c: r == c + 64)
    high_high = picker(128, 128, lambda r, c: (r == c) & (c >= 64))
    return (low_low, low_high), (high_low, high_high)


def mixer_kernel(
    q_ref, k_ref, v_ref, shift_ref, head_shift_ref, stream_ref, mix_ref, w_ref, post_ref,
    hidden_ref,
    sendbuf, recvbuf, attsend, attrecv, qs, kk, vv, off, w_vmem, normed,
    send_sem, recv_sem, asend_sem, arecv_sem, w_sem,
):
    me = lax.axis_index("sp")
    barrier = pltpu.get_barrier_semaphore()
    for d in range(1, 16):
        pl.semaphore_signal(
            barrier, inc=1, device_id={"sp": lax.rem(me + d, 16)}, device_id_type=pl.DeviceIdType.MESH
        )
    w_copy = pltpu.make_async_copy(w_ref, w_vmem, w_sem)
    w_copy.start()

    pickers = half_pickers()
    shifts = lax.dot_general(
        picker(16, 16, lambda r, c: r == c), shift_ref[...], NT, preferred_element_type=F32
    )
    for h in range(16):
        tile = slice((h // 2) * 128, (h // 2 + 1) * 128)
        first, second = pickers[h % 2]
        sendbuf[h, 0:128, :] = (f32dot(q_ref[:, tile], first) + f32dot(k_ref[:, tile], second)).astype(BF16)
        sendbuf[h, 128:192, :] = (
            f32dot(v_ref[0:64, tile], first) + f32dot(v_ref[64:128, tile], second)
        ).astype(BF16)
        sendbuf[h, 192:208, :] = jnp.broadcast_to(shifts[h:h + 1, :], (16, 128)).astype(BF16)

    pl.semaphore_wait(barrier, 15)

    def outgoing(d):
        to = lax.rem(me + d, 16)
        return pltpu.make_async_remote_copy(
            src_ref=sendbuf.at[to],
            dst_ref=recvbuf.at[me],
            send_sem=send_sem.at[d],
            recv_sem=recv_sem.at[d],
            device_id={"sp": to},
            device_id_type=pl.DeviceIdType.MESH,
        )

    for d in range(1, 16):
        outgoing(d).start()
    recvbuf[me] = sendbuf[me]
    for d in range(1, 16):
        outgoing(d).wait()

    both_low = picker(128, 128, lambda r, c: r == c % 64)
    both_high = picker(128, 128, lambda r, c: r == c % 64 + 64)
    lane = lax.broadcasted_iota(jnp.int32, (128, 128), 1)
    hs = head_shift_ref[0]
    for j in range(16):
        rows = slice(j * 128, (j + 1) * 128)
        qk = recvbuf[j, 0:128, :]
        q2 = f32dot(qk, both_low) * (LOG2E / 8.0)
        hi = q2.astype(BF16).astype(F32)
        qs[rows, :] = jnp.where(lane < 64, hi, q2 - hi).astype(BF16)
        kk[rows, :] = f32dot(qk, both_high).astype(BF16)
        vm = recvbuf[j, 128:192, :]
        vv[j * 128:j * 128 + 64, :] = f32dot(vm, both_low).astype(BF16)
        vv[j * 128 + 64:j * 128 + 128, :] = f32dot(vm, both_high).astype(BF16)
        off[0:1, rows] = (recvbuf[j, 192:208, :].astype(F32)[0:1] + hs) * LOG2E

    tri = picker(KB, KB, lambda r, c: r >= c)
    lane64 = lax.broadcasted_iota(jnp.int32, (64, 128), 1) < 64

    def reply(j):
        return pltpu.make_async_remote_copy(
            src_ref=attsend.at[j],
            dst_ref=attrecv.at[me],
            send_sem=asend_sem.at[j],
            recv_sem=arecv_sem.at[me],
            device_id={"sp": j},
            device_id_type=pl.DeviceIdType.MESH,
        )

    for qi in range(2048 // QB):
        r0 = qi * QB
        carry = jnp.zeros((QB, 1), F32)
        acc = jnp.zeros((QB, 128), F32)
        for ki in range(qi, -1, -1):
            k0 = ki * KB
            z = lax.dot_general(qs[r0:r0 + QB, :], kk[k0:k0 + KB, :], NT, preferred_element_type=F32)
            z = z + off[0:1, k0:k0 + KB]
            sp = jnp.maximum(z, jnp.log2(1.0 + jnp.exp2(jnp.minimum(z, 100.0))))
            if ki == qi:
                r = lax.broadcasted_iota(jnp.int32, (QB, KB), 0)
                c = lax.broadcasted_iota(jnp.int32, (QB, KB), 1)
                sp = jnp.where(c < r, sp, 0.0)
            hi = sp.astype(BF16)
            lo = (sp - hi.astype(F32)).astype(BF16)
            s = f32dot(hi, tri) + f32dot(lo, tri)
            w = jnp.exp2(z - (s + carry))
            if ki == qi:
                w = jnp.where(c < r, w, 0.0)
            acc = acc + f32dot(w.astype(BF16), vv[k0:k0 + KB, :])
            carry = carry + s[:, 0:1]
        for part in range(QB // 128):
            j = r0 // 128 + part
            at = part * 128
            attsend[j] = jnp.where(lane64, acc[at:at + 64], acc[at + 64:at + 128]).astype(BF16)

            @pl.when(me != j)
            def _():
                reply(j).start()

            @pl.when(me == j)
            def _():
                attrecv[j] = attsend[j]

    for j in range(16):
        @pl.when(me != j)
        def _():
            reply(j).wait_send()
            pltpu.make_async_remote_copy(
                src_ref=attsend.at[j],
                dst_ref=attrecv.at[j],
                send_sem=asend_sem.at[j],
                recv_sem=arecv_sem.at[j],
                device_id={"sp": j},
                device_id_type=pl.DeviceIdType.MESH,
            ).wait_recv()

    (low_low, low_high), (high_low, high_high) = pickers
    squares = jnp.zeros((128, 1), F32)
    tiles = []
    for p in range(8):
        even, odd = attrecv[2 * p], attrecv[2 * p + 1]
        low = f32dot(even, low_low) + f32dot(odd, low_high)
        high = f32dot(even, high_low) + f32dot(odd, high_high)
        tile = jnp.concatenate([low, high], axis=0)
        squares = squares + jnp.sum(tile * tile, axis=1, keepdims=True)
        tiles.append(tile)
    inv = lax.rsqrt(squares * (1.0 / 1024.0) + norm_eps)
    for p in range(8):
        cols = slice(p * 128, (p + 1) * 128)
        normed[:, cols] = (tiles[p] * inv * mix_ref[:, cols]).astype(BF16)
    w_copy.wait()
    totals = jnp.zeros((128, 1), F32)
    sums = []
    for n in range(8):
        cols = slice(n * 256, (n + 1) * 256)
        summed = stream_ref[:, cols].astype(F32) + f32dot(normed[...], w_vmem[:, cols])
        totals = totals + jnp.sum(summed * summed, axis=1, keepdims=True)
        sums.append(summed)
    inv = lax.rsqrt(totals * (1.0 / 2048.0) + norm_eps)
    for n in range(8):
        cols = slice(n * 256, (n + 1) * 256)
        hidden_ref[:, cols] = (sums[n] * inv * post_ref[:, cols]).astype(BF16)


def mixer(q, k, v, shift, head_shift, stream, mix_gain, out_weight, post_gain):
    vmem = pl.BlockSpec(memory_space=pltpu.VMEM)
    return pl.pallas_call(
        mixer_kernel,
        out_shape=jax.ShapeDtypeStruct((128, 2048), BF16),
        in_specs=[vmem] * 4 + [pl.BlockSpec(memory_space=pltpu.SMEM)] + [vmem] * 2
        + [pl.BlockSpec(memory_space=pl.ANY), vmem],
        out_specs=vmem,
        scratch_shapes=[
            pltpu.VMEM((16, 208, 128), BF16),
            pltpu.VMEM((16, 208, 128), BF16),
            pltpu.VMEM((16, 64, 128), BF16),
            pltpu.VMEM((16, 64, 128), BF16),
            pltpu.VMEM((2048, 128), BF16),
            pltpu.VMEM((2048, 128), BF16),
            pltpu.VMEM((2048, 128), BF16),
            pltpu.VMEM((8, 2048), F32),
            pltpu.VMEM((1024, 2048), BF16),
            pltpu.VMEM((128, 1024), BF16),
            pltpu.SemaphoreType.DMA((16,)),
            pltpu.SemaphoreType.DMA((16,)),
            pltpu.SemaphoreType.DMA((16,)),
            pltpu.SemaphoreType.DMA((16,)),
            pltpu.SemaphoreType.DMA,
        ],
        compiler_params=pltpu.CompilerParams(
            collective_id=1, has_side_effects=True, vmem_limit_bytes=56 * 2**20
        ),
    )(q, k, v, shift, head_shift, stream, mix_gain, out_weight, post_gain)


CHUNKS = 4
CW = 2048 // CHUNKS
STEP = 11


def row_iota(rows, cols):
    return lax.broadcasted_iota(jnp.int32, (rows, cols), 0)


def col_iota(rows, cols):
    return lax.broadcasted_iota(jnp.int32, (rows, cols), 1)


def as_whole(x):
    return x.astype(jnp.int32)


def moe_kernel(
    hidden_ref, route_ref, weight_ref, gate_hbm, up_hbm, down_hbm,
    out_ref,
    msend, mrecv, zsend, zrecv, psend, precv, osend, oret, ysend, yback,
    gate_w, up_w, down_w, gate_acc, up_acc, inner,
    m_ss, m_rs, z_ss, z_rs, p_ss, p_rs, o_ss, o_rs, y_ss, y_rs, w_sem,
):
    sp, dp = lax.axis_index("sp"), lax.axis_index("dp")
    z, y = sp // 4, lax.rem(sp, 4)
    place = y * 8 + dp

    def on_z(at):
        return {"sp": at * 4 + y}

    def in_plane(p):
        return {"sp": z * 4 + p // 8, "dp": lax.rem(p, 8)}

    def plane_peer(i):
        o = lax.rem(i * STEP, 32)
        py = lax.rem(place // 8 + o // 8, 4)
        px = lax.rem(lax.rem(place, 8) // 2 + lax.rem(o, 8) // 2, 4)
        pc = lax.rem(place + o, 2)
        return py * 8 + px * 2 + pc

    mesh_id = pl.DeviceIdType.MESH
    barrier = pltpu.get_barrier_semaphore()
    for d in range(1, 4):
        pl.semaphore_signal(barrier, inc=1, device_id=on_z(lax.rem(z + d, 4)), device_id_type=mesh_id)

    def greet(i, _):
        pl.semaphore_signal(barrier, inc=1, device_id=in_plane(plane_peer(i)), device_id_type=mesh_id)
        return 0

    lax.fori_loop(1, 32, greet, 0)
    copies = [
        pltpu.make_async_copy(a, b, w_sem.at[i])
        for i, (a, b) in enumerate(((gate_hbm, gate_w), (up_hbm, up_w), (down_hbm, down_w)))
    ]
    for c in copies:
        c.start()

    lanes = col_iota(128, 128)
    first, second = route_ref[:, 0:1], route_ref[:, 1:2]
    in_first = jnp.where(lanes == first, 1.0, 0.0)
    in_second = jnp.where(lanes == second, 1.0, 0.0)
    before = picker(128, 128, lambda r, c: c < r)
    named = f32dot(before, (in_first + in_second).astype(BF16))
    rank_first = jnp.sum(in_first * named, axis=1, keepdims=True)
    rank_second = jnp.sum(in_second * named, axis=1, keepdims=True)
    group = lax.shift_right_logical(first, 5)
    in_group = jnp.where(lanes == group, 1.0, 0.0)
    within = jnp.sum(in_group * f32dot(before, in_group.astype(BF16)), axis=1, keepdims=True)
    w0, w1 = weight_ref[:, 0:1], weight_ref[:, 1:2]
    w0_hi, w1_hi = w0.astype(BF16).astype(F32), w1.astype(BF16).astype(F32)
    fields = (
        ((first & 31) + 1).astype(F32), rank_first, ((second & 31) + 1).astype(F32), rank_second,
        w0_hi, w0 - w0_hi, w1_hi, w1 - w1_hi, group.astype(F32), within,
    )
    table = jnp.zeros((128, 128), F32)
    for i, field in enumerate(fields):
        table = jnp.where(lanes == i, field, table)
    table = table.astype(BF16)
    eye = picker(16, 128, lambda r, c: r == c)
    by_lane = lax.dot_general(eye, table, NT, preferred_element_type=F32)
    goes_to = as_whole(by_lane[8:9] * 64.0 + by_lane[9:10])
    to_plane = jnp.where(row_iota(256, 128) == goes_to, 1.0, 0.0).astype(BF16)
    from_plane = jnp.where(
        col_iota(128, 256) == group * 64 + as_whole(within), 1.0, 0.0
    ).astype(BF16)
    msend[...] = f32dot(to_plane, table).astype(BF16).reshape(4, 64, 128)

    pl.semaphore_wait(barrier, 34)

    def z_copy(src, dst, ss, rs, d, c=None):
        to = lax.rem(z + d, 4)
        return pltpu.make_async_remote_copy(
            src_ref=src.at[to] if c is None else src.at[c, to],
            dst_ref=dst.at[z] if c is None else dst.at[c, z],
            send_sem=ss.at[d] if c is None else ss.at[c, d],
            recv_sem=rs.at[d] if c is None else rs.at[c, d],
            device_id=on_z(to),
            device_id_type=mesh_id,
        )

    def p_copy(src, dst, ss, rs, i, c):
        to = plane_peer(i)
        return pltpu.make_async_remote_copy(
            src_ref=src.at[c, to],
            dst_ref=dst.at[c, place],
            send_sem=ss.at[c, i],
            recv_sem=rs.at[c, i],
            device_id=in_plane(to),
            device_id_type=mesh_id,
        )

    def p_start(src, dst, ss, rs, c):
        def one(i, _):
            p_copy(src, dst, ss, rs, i, c).start()
            return 0

        lax.fori_loop(1, 32, one, 0)
        dst[c, place] = src[c, place]

    def p_wait(src, dst, ss, rs, c):
        def one(i, _):
            p_copy(src, dst, ss, rs, i, c).wait_recv()
            return 0

        lax.fori_loop(1, 32, one, 0)

    for d in range(1, 4):
        z_copy(msend, mrecv, m_ss, m_rs, d).start()
    mrecv[z] = msend[z]
    for c in range(CHUNKS):
        cols = slice(c * CW, (c + 1) * CW)
        zsend[c] = f32dot(to_plane, hidden_ref[:, cols]).astype(BF16).reshape(4, 64, CW)
        for d in range(1, 4):
            z_copy(zsend, zrecv, z_ss, z_rs, d, c).start()
        zrecv[c, z] = zsend[c, z]

    for d in range(1, 4):
        z_copy(msend, mrecv, m_ss, m_rs, d).wait_recv()
    got = mrecv[...].reshape(256, 128)
    by_lane = lax.dot_general(eye, got, NT, preferred_element_type=F32)
    by_row = got.astype(F32)

    def slots(p, rank, source):
        at = (as_whole(p) - 1) * 16 + source * 4 + as_whole(rank)
        return jnp.where(p > 0.5, at, -1)

    source = lax.shift_right_logical(col_iota(1, 256), 6)
    slot0, slot1 = slots(by_lane[0:1], by_lane[1:2], source), slots(by_lane[2:3], by_lane[3:4], source)
    at = row_iota(512, 256)
    to_experts = jnp.where((at == slot0) | (at == slot1), 1.0, 0.0).astype(BF16)
    source = lax.shift_right_logical(row_iota(256, 1), 6)
    slot0 = slots(by_row[:, 0:1], by_row[:, 1:2], source)
    slot1 = slots(by_row[:, 2:3], by_row[:, 3:4], source)
    at = col_iota(256, 512)
    is0, is1 = at == slot0, at == slot1
    mix_hi = jnp.where(is0, by_row[:, 4:5], jnp.where(is1, by_row[:, 6:7], 0.0)).astype(BF16)
    mix_lo = jnp.where(is0, by_row[:, 5:6], jnp.where(is1, by_row[:, 7:8], 0.0)).astype(BF16)

    for c in range(CHUNKS):
        for d in range(1, 4):
            z_copy(zsend, zrecv, z_ss, z_rs, d, c).wait_recv()
        psend[c] = f32dot(to_experts, zrecv[c].reshape(256, CW)).astype(BF16).reshape(32, 16, CW)
        p_start(psend, precv, p_ss, p_rs, c)

    for i in range(2):
        copies[i].wait()
    for c in range(CHUNKS):
        p_wait(psend, precv, p_ss, p_rs, c)
        rows = precv[c].reshape(512, CW)
        deep = slice(c * CW, (c + 1) * CW)

        def expert_in(n, _):
            cols = pl.ds(pl.multiple_of(n * 256, 256), 256)
            g = f32dot(rows, gate_w[deep, cols])
            u = f32dot(rows, up_w[deep, cols])
            if c > 0:
                g = g + gate_acc[:, cols]
                u = u + up_acc[:, cols]
            if c < CHUNKS - 1:
                gate_acc[:, cols] = g
                up_acc[:, cols] = u
            else:
                inner[:, cols] = (g / (1.0 + jnp.exp(-g)) * u).astype(BF16)
            return 0

        lax.fori_loop(0, 4, expert_in, 0)

    copies[2].wait()
    for c in range(CHUNKS):
        def expert_out(n, _):
            cols = pl.ds(pl.multiple_of(n * 256, 256), 256)
            o = f32dot(inner[...], down_w[:, pl.ds(pl.multiple_of(c * CW + n * 256, 256), 256)])
            osend[c, :, :, cols] = o.astype(BF16).reshape(32, 16, 256)
            return 0

        lax.fori_loop(0, CW // 256, expert_out, 0)
        p_start(osend, oret, o_ss, o_rs, c)

    for c in range(CHUNKS):
        p_wait(osend, oret, o_ss, o_rs, c)
        rows = oret[c].reshape(512, CW)
        part = f32dot(mix_hi, rows) + f32dot(mix_lo, rows)
        ysend[c] = part.astype(BF16).reshape(4, 64, CW)
        for d in range(1, 4):
            z_copy(ysend, yback, y_ss, y_rs, d, c).start()
        yback[c, z] = ysend[c, z]

    for c in range(CHUNKS):
        for d in range(1, 4):
            z_copy(ysend, yback, y_ss, y_rs, d, c).wait_recv()
        cols = slice(c * CW, (c + 1) * CW)
        moe = f32dot(from_plane, yback[c].reshape(256, CW))
        out_ref[:, cols] = (hidden_ref[:, cols].astype(F32) + moe).astype(BF16)

    for d in range(1, 4):
        z_copy(msend, mrecv, m_ss, m_rs, d).wait_send()
        for c in range(CHUNKS):
            z_copy(zsend, zrecv, z_ss, z_rs, d, c).wait_send()
            z_copy(ysend, yback, y_ss, y_rs, d, c).wait_send()

    def sent(i, _):
        for c in range(CHUNKS):
            p_copy(psend, precv, p_ss, p_rs, i, c).wait_send()
            p_copy(osend, oret, o_ss, o_rs, i, c).wait_send()
        return 0

    lax.fori_loop(1, 32, sent, 0)


def moe(hidden, route, route_weight, w_gate, w_up, w_down):
    vmem = pl.BlockSpec(memory_space=pltpu.VMEM)
    dma = pltpu.SemaphoreType.DMA
    return pl.pallas_call(
        moe_kernel,
        out_shape=jax.ShapeDtypeStruct((128, 2048), BF16),
        in_specs=[vmem] * 3 + [pl.BlockSpec(memory_space=pl.ANY)] * 3,
        out_specs=vmem,
        scratch_shapes=[pltpu.VMEM((4, 64, 128), BF16)] * 2
        + [pltpu.VMEM((CHUNKS, 4, 64, CW), BF16)] * 2
        + [pltpu.VMEM((CHUNKS, 32, 16, CW), BF16)] * 4
        + [pltpu.VMEM((CHUNKS, 4, 64, CW), BF16)] * 2
        + [pltpu.VMEM((2048, 1024), BF16)] * 2
        + [pltpu.VMEM((1024, 2048), BF16)]
        + [pltpu.VMEM((512, 1024), F32)] * 2
        + [pltpu.VMEM((512, 1024), BF16)]
        + [dma((4,))] * 2
        + [dma((CHUNKS, 4))] * 2
        + [dma((CHUNKS, 32))] * 4
        + [dma((CHUNKS, 4))] * 2
        + [dma((3,))],
        compiler_params=pltpu.CompilerParams(
            collective_id=2, has_side_effects=True, vmem_limit_bytes=58 * 2**20
        ),
    )(hidden, route, route_weight, w_gate, w_up, w_down)


def on_device(
    stream,
    queries,
    keys_in,
    values_in,
    key_shift,
    head_shift,
    mix_gain,
    out_weight,
    post_gain,
    route,
    route_weight,
    w_gate,
    w_up,
    w_down,
):
    own_shift = lax.dynamic_slice_in_dim(head_shift, lax.axis_index(SP), 1)
    hidden = mixer(
        queries[0], keys_in[0], values_in[0], key_shift[0], own_shift, stream[0],
        mix_gain[None], out_weight, post_gain[None],
    )
    result = moe(hidden, route[0], route_weight[0], w_gate[0], w_up[0], w_down[0])
    return result[None]


def solution(mesh):
    placed = (
        P("dp", SP, None),
        P("dp", SP, None),
        P("dp", SP, None),
        P("dp", SP, None),
        P("dp", SP, None),
        P(),
        P(),
        P(),
        P(),
        P("dp", SP, None),
        P("dp", SP, None),
        P(SP_DP, None, None),
        P(SP_DP, None, None),
        P(SP_DP, None, None),
    )
    return jax.shard_map(
        on_device, mesh=mesh, in_specs=placed, out_specs=P("dp", SP, None), check_vma=False
    )
```

```python
import jax
import jax.numpy as jnp
from jax import lax
from jax.sharding import PartitionSpec as P
from jax.experimental import pallas as pl
from jax.experimental.pallas import tpu as pltpu

SP = "sp"
SP_DP = ("sp", "dp")
norm_eps = 1e-05
STEP = 11
CW = 512
OFFSETS = (1, 3, 2)
WIDE = 512

LOG2E = 1.4426950408889634
KB = 256
QB = 512
NT = (((1,), (1,)), ((), ()))
BF16 = jnp.bfloat16
F32 = jnp.float32


def picker(rows, cols, fn):
    r = lax.broadcasted_iota(jnp.int32, (rows, cols), 0)
    c = lax.broadcasted_iota(jnp.int32, (rows, cols), 1)
    return jnp.where(fn(r, c), 1.0, 0.0).astype(BF16)


def f32dot(a, b):
    return jnp.dot(a, b, preferred_element_type=F32)


def half_pickers():
    low_low = picker(128, 128, lambda r, c: (r == c) & (c < 64))
    low_high = picker(128, 128, lambda r, c: r == c - 64)
    high_low = picker(128, 128, lambda r, c: r == c + 64)
    high_high = picker(128, 128, lambda r, c: (r == c) & (c >= 64))
    return (low_low, low_high), (high_low, high_high)


def row_iota(rows, cols):
    return lax.broadcasted_iota(jnp.int32, (rows, cols), 0)


def col_iota(rows, cols):
    return lax.broadcasted_iota(jnp.int32, (rows, cols), 1)


def as_whole(x):
    return x.astype(jnp.int32)


def layer_kernel(
    q_hbm, k_hbm, v_hbm, shift_ref, head_shift_ref, stream_hbm, mix_ref, w_hbm, post_ref,
    route_ref, weight_ref, gate_hbm, up_hbm, down_hbm,
    out_ref,
    q_ref, k_ref, v_ref, stream_ref, w_vmem, hidden_ref,
    sendbuf, recvbuf, attsend, attrecv, qs, kk, vv, off, normed,
    to_plane, from_plane, to_experts, mix_hi, mix_lo, spread, gather,
    msend, mrecv, zsend, zrecv, psend, precv, osend, oret, ysend, yback,
    gate_w, up_w, down_w, xs, inner, outs,
    send_sem, recv_sem, asend_sem, arecv_sem,
    m_ss, m_rs, z_ss, z_rs, p_ss, p_rs, o_ss, o_rs, y_ss, y_rs, load_sem,
):
    me, dp = lax.axis_index("sp"), lax.axis_index("dp")
    z, y = me // 4, lax.rem(me, 4)
    place = y * 8 + dp
    mesh_id = pl.DeviceIdType.MESH

    def on_z(at):
        return {"sp": at * 4 + y}

    def in_plane(p):
        return {"sp": z * 4 + p // 8, "dp": lax.rem(p, 8)}

    def plane_peer(i):
        o = lax.rem(i * STEP, 32)
        py = lax.rem(place // 8 + o // 8, 4)
        px = lax.rem(lax.rem(place, 8) // 2 + lax.rem(o, 8) // 2, 4)
        pc = lax.rem(place + o, 2)
        return py * 8 + px * 2 + pc

    def sp_peer(d):
        return lax.rem(me + d, 16)

    barrier = pltpu.get_barrier_semaphore()

    def greet_sp(d, _):
        pl.semaphore_signal(barrier, inc=1, device_id={"sp": sp_peer(d)}, device_id_type=mesh_id)
        return 0

    def greet_plane(i, _):
        pl.semaphore_signal(barrier, inc=1, device_id=in_plane(plane_peer(i)), device_id_type=mesh_id)
        return 0

    lax.fori_loop(1, 16, greet_sp, 0)
    lax.fori_loop(1, 32, greet_plane, 0)
    loads = [
        pltpu.make_async_copy(a, b, load_sem.at[i])
        for i, (a, b) in enumerate((
            (q_hbm, q_ref), (k_hbm, k_ref), (v_hbm, v_ref), (stream_hbm, stream_ref),
            (w_hbm, w_vmem), (gate_hbm, gate_w), (up_hbm, up_w), (down_hbm, down_w),
        ))
    ]
    for c in loads:
        c.start()
    q_load, k_load, v_load, stream_load, w_load, gate_load, up_load, down_load = loads

    lanes = col_iota(128, 128)
    w_row = weight_ref[...]
    w_hi = w_row.astype(BF16).astype(F32)
    facts = jnp.concatenate(
        [route_ref[...].astype(F32), w_hi, w_row - w_hi, jnp.zeros((10, 128), F32)], axis=0
    ).astype(BF16)
    whole_eye = picker(128, 128, lambda r, c: r == c)
    by_token = lax.dot_general(whole_eye, facts, NT, preferred_element_type=F32)
    first, second = as_whole(by_token[:, 0:1]), as_whole(by_token[:, 1:2])
    in_first = jnp.where(lanes == first, 1.0, 0.0)
    in_second = jnp.where(lanes == second, 1.0, 0.0)
    before = picker(128, 128, lambda r, c: c < r)
    named = f32dot(before, (in_first + in_second).astype(BF16))
    rank_first = jnp.sum(in_first * named, axis=1, keepdims=True)
    rank_second = jnp.sum(in_second * named, axis=1, keepdims=True)
    group = (lax.shift_right_logical(first, 5) - z) & 3
    in_group = jnp.where(lanes == group, 1.0, 0.0)
    within = jnp.sum(in_group * f32dot(before, in_group.astype(BF16)), axis=1, keepdims=True)
    fields = (
        ((first & 31) + 1).astype(F32), rank_first, ((second & 31) + 1).astype(F32), rank_second,
        by_token[:, 2:3], by_token[:, 4:5], by_token[:, 3:4], by_token[:, 5:6], group.astype(F32), within,
    )
    table = jnp.zeros((128, 128), F32)
    for i, field in enumerate(fields):
        table = jnp.where(lanes == i, field, table)
    table = table.astype(BF16)
    eye = picker(16, 128, lambda r, c: r == c)
    by_lane = lax.dot_general(eye, table, NT, preferred_element_type=F32)
    goes_to = as_whole(by_lane[8:9] * 64.0 + by_lane[9:10])
    to_plane[...] = jnp.where(row_iota(256, 128) == goes_to, 1.0, 0.0).astype(BF16)
    from_plane[...] = jnp.where(
        col_iota(128, 256) == group * 64 + as_whole(within), 1.0, 0.0
    ).astype(BF16)
    msend[...] = f32dot(to_plane[...], table).astype(BF16).reshape(4, 64, 128)

    pickers = half_pickers()
    shifts = shift_ref[...].astype(F32)
    q_load.wait()
    k_load.wait()
    v_load.wait()
    for h in range(16):
        tile = slice((h // 2) * 128, (h // 2 + 1) * 128)
        first, second = pickers[h % 2]
        sendbuf[h, 0:128, :] = (f32dot(q_ref[:, tile], first) + f32dot(k_ref[:, tile], second)).astype(BF16)
        sendbuf[h, 128:192, :] = (
            f32dot(v_ref[0:64, tile], first) + f32dot(v_ref[64:128, tile], second)
        ).astype(BF16)
        sendbuf[h, 192:208, :] = jnp.broadcast_to(shifts[h:h + 1, :], (16, 128)).astype(BF16)

    pl.semaphore_wait(barrier, 46)

    def z_copy(src, dst, ss, rs, d, way=1):
        return pltpu.make_async_remote_copy(
            src_ref=src.at[d],
            dst_ref=dst.at[d],
            send_sem=ss.at[d],
            recv_sem=rs.at[d],
            device_id=on_z(lax.rem(z + 4 + way * d, 4)),
            device_id_type=mesh_id,
        )

    def p_copy(src, dst, ss, rs, i, d):
        to = plane_peer(i)
        return pltpu.make_async_remote_copy(
            src_ref=src.at[d, to],
            dst_ref=dst.at[d, place],
            send_sem=ss.at[d, i],
            recv_sem=rs.at[d, i],
            device_id=in_plane(to),
            device_id_type=mesh_id,
        )

    def p_start(src, dst, ss, rs, d):
        def one(i, _):
            p_copy(src, dst, ss, rs, i, d).start()
            return 0

        lax.fori_loop(1, 32, one, 0)
        dst[d, place] = src[d, place]

    def p_wait(src, dst, ss, rs, d):
        def one(i, _):
            p_copy(src, dst, ss, rs, i, d).wait_recv()
            return 0

        lax.fori_loop(1, 32, one, 0)

    def outgoing(d):
        to = sp_peer(d)
        return pltpu.make_async_remote_copy(
            src_ref=sendbuf.at[to],
            dst_ref=recvbuf.at[me],
            send_sem=send_sem.at[d],
            recv_sem=recv_sem.at[d],
            device_id={"sp": to},
            device_id_type=pl.DeviceIdType.MESH,
        )

    for d in range(1, 16):
        outgoing(d).start()
    recvbuf[me] = sendbuf[me]
    for d in range(1, 4):
        z_copy(msend, mrecv, m_ss, m_rs, d).start()
    mrecv[0] = msend[0]

    for d in range(1, 4):
        z_copy(msend, mrecv, m_ss, m_rs, d).wait_recv()
    def slots(p, rank, quarter):
        at = (as_whole(p) - 1) * 16 + quarter * 4 + as_whole(rank)
        return jnp.where(p > 0.5, at, -1)

    lane_quarter = lax.shift_right_logical(col_iota(1, 256), 6)
    row_quarter = lax.shift_right_logical(row_iota(256, 1), 6)
    for d in range(4):
        got = jnp.concatenate([mrecv[d]] * 4, axis=0)
        by_lane = lax.dot_general(eye, got, NT, preferred_element_type=F32)
        by_row = got.astype(F32)
        slot0 = slots(by_lane[0:1], by_lane[1:2], lane_quarter)
        slot1 = slots(by_lane[2:3], by_lane[3:4], lane_quarter)
        at = row_iota(512, 256)
        to_experts[d] = jnp.where((at == slot0) | (at == slot1), 1.0, 0.0).astype(BF16)
        slot0 = slots(by_row[:, 0:1], by_row[:, 1:2], row_quarter)
        slot1 = slots(by_row[:, 2:3], by_row[:, 3:4], row_quarter)
        at = col_iota(256, 512)
        is0, is1 = at == slot0, at == slot1
        mix_hi[d] = jnp.where(is0, by_row[:, 4:5], jnp.where(is1, by_row[:, 6:7], 0.0)).astype(BF16)
        mix_lo[d] = jnp.where(is0, by_row[:, 5:6], jnp.where(is1, by_row[:, 7:8], 0.0)).astype(BF16)

    def message_row(stacked):
        return (stacked & 127) // 4 * 16 + lax.shift_right_logical(stacked, 7) * 4 + (stacked & 3)

    spread[...] = jnp.where(row_iota(512, 512) == message_row(col_iota(1, 512)), 1.0, 0.0).astype(BF16)
    gather[...] = jnp.where(col_iota(512, 512) == message_row(row_iota(512, 1)), 1.0, 0.0).astype(BF16)

    for d in range(1, 16):
        outgoing(d).wait()

    both_low = picker(128, 128, lambda r, c: r == c % 64)
    both_high = picker(128, 128, lambda r, c: r == c % 64 + 64)
    lane = lax.broadcasted_iota(jnp.int32, (128, 128), 1)
    hs = head_shift_ref[me]
    for j in range(16):
        rows = slice(j * 128, (j + 1) * 128)
        qk = recvbuf[j, 0:128, :]
        q2 = f32dot(qk, both_low) * (LOG2E / 8.0)
        hi = q2.astype(BF16).astype(F32)
        qs[rows, :] = jnp.where(lane < 64, hi, q2 - hi).astype(BF16)
        kk[rows, :] = f32dot(qk, both_high).astype(BF16)
        vm = recvbuf[j, 128:192, :]
        vv[j * 128:j * 128 + 64, :] = f32dot(vm, both_low).astype(BF16)
        vv[j * 128 + 64:j * 128 + 128, :] = f32dot(vm, both_high).astype(BF16)
        off[0:1, rows] = (recvbuf[j, 192:208, :].astype(F32)[0:1] + hs) * LOG2E

    tri = picker(KB, KB, lambda r, c: r >= c)
    lane64 = lax.broadcasted_iota(jnp.int32, (64, 128), 1) < 64

    def reply(j):
        return pltpu.make_async_remote_copy(
            src_ref=attsend.at[j],
            dst_ref=attrecv.at[me],
            send_sem=asend_sem.at[j],
            recv_sem=arecv_sem.at[me],
            device_id={"sp": j},
            device_id_type=pl.DeviceIdType.MESH,
        )

    for qi in range(2048 // QB):
        r0 = qi * QB
        carry = jnp.zeros((QB, 1), F32)
        acc = jnp.zeros((QB, 128), F32)
        for ki in range((r0 + QB) // KB - 1, -1, -1):
            k0 = ki * KB
            logit = lax.dot_general(qs[r0:r0 + QB, :], kk[k0:k0 + KB, :], NT, preferred_element_type=F32)
            logit = logit + off[0:1, k0:k0 + KB]
            sp = jnp.maximum(logit, jnp.log2(1.0 + jnp.exp2(jnp.minimum(logit, 100.0))))
            masked = k0 >= r0
            if masked:
                r = lax.broadcasted_iota(jnp.int32, (QB, KB), 0)
                c = lax.broadcasted_iota(jnp.int32, (QB, KB), 1)
                earlier = c - r < r0 - k0
                sp = jnp.where(earlier, sp, 0.0)
            hi = sp.astype(BF16)
            lo = (sp - hi.astype(F32)).astype(BF16)
            s = f32dot(hi, tri) + f32dot(lo, tri)
            w = jnp.exp2((logit - s) - carry)
            if masked:
                w = jnp.where(earlier, w, 0.0)
            acc = acc + f32dot(w.astype(BF16), vv[k0:k0 + KB, :])
            carry = carry + s[:, 0:1]
        for part in range(QB // 128):
            j = r0 // 128 + part
            at = part * 128
            attsend[j] = jnp.where(lane64, acc[at:at + 64], acc[at + 64:at + 128]).astype(BF16)

            @pl.when(me != j)
            def _():
                reply(j).start()

            @pl.when(me == j)
            def _():
                attrecv[j] = attsend[j]

    for j in range(16):
        @pl.when(me != j)
        def _():
            reply(j).wait_send()
            pltpu.make_async_remote_copy(
                src_ref=attsend.at[j],
                dst_ref=attrecv.at[j],
                send_sem=asend_sem.at[j],
                recv_sem=arecv_sem.at[j],
                device_id={"sp": j},
                device_id_type=pl.DeviceIdType.MESH,
            ).wait_recv()

    (low_low, low_high), (high_low, high_high) = pickers
    squares = jnp.zeros((128, 1), F32)
    tiles = []
    for p in range(8):
        even, odd = attrecv[2 * p], attrecv[2 * p + 1]
        low = f32dot(even, low_low) + f32dot(odd, low_high)
        high = f32dot(even, high_low) + f32dot(odd, high_high)
        tile = jnp.concatenate([low, high], axis=0)
        squares = squares + jnp.sum(tile * tile, axis=1, keepdims=True)
        tiles.append(tile)
    inv = lax.rsqrt(squares * (1.0 / 1024.0) + norm_eps)
    for p in range(8):
        cols = slice(p * 128, (p + 1) * 128)
        normed[:, cols] = (tiles[p] * inv * mix_ref[:, cols]).astype(BF16)
    w_load.wait()
    stream_load.wait()
    totals = jnp.zeros((128, 1), F32)
    sums = []
    for n in range(8):
        cols = slice(n * 256, (n + 1) * 256)
        summed = stream_ref[:, cols].astype(F32) + f32dot(normed[...], w_vmem[:, cols])
        totals = totals + jnp.sum(summed * summed, axis=1, keepdims=True)
        sums.append(summed)
    inv = lax.rsqrt(totals * (1.0 / 2048.0) + norm_eps)
    for n in range(8):
        cols = slice(n * 256, (n + 1) * 256)
        hidden_ref[:, cols] = (sums[n] * inv * post_ref[:, cols]).astype(BF16)

    for q in range(4):
        rows = f32dot(to_plane[...], hidden_ref[:, q * CW:(q + 1) * CW]).astype(BF16)
        for d in range(4):
            zsend[d, q] = rows[d * 64:(d + 1) * 64]
    for d in OFFSETS:
        z_copy(zsend, zrecv, z_ss, z_rs, d).start()

    def dispatch(d, source):
        if d:
            z_copy(zsend, zrecv, z_ss, z_rs, d).wait_recv()
        psend[d] = f32dot(to_experts[d], source[d].reshape(256, CW)).astype(BF16).reshape(32, 16, CW)
        p_start(psend, precv, p_ss, p_rs, d)

    def expert(d):
        p_wait(psend, precv, p_ss, p_rs, d)
        stacked = f32dot(gather[...], precv[d].reshape(512, CW)).astype(BF16)
        for q in range(4):
            xs[:, q * CW:(q + 1) * CW] = stacked[q * 128:(q + 1) * 128]

        def first_half(n, _):
            cols = pl.ds(pl.multiple_of(n * WIDE, WIDE), WIDE)
            g = f32dot(xs[...], gate_w[:, cols])
            u = f32dot(xs[...], up_w[:, cols])
            inner[:, cols] = (g / (1.0 + jnp.exp(-g)) * u).astype(BF16)
            return 0

        lax.fori_loop(0, 1024 // WIDE, first_half, 0)

        def second_half(q, _):
            cols = pl.ds(pl.multiple_of(q * CW, CW), CW)
            outs[q] = f32dot(inner[...], down_w[:, cols]).astype(BF16)
            return 0

        lax.fori_loop(0, 4, second_half, 0)
        osend[d] = f32dot(spread[...], outs[...].reshape(512, CW)).astype(BF16).reshape(32, 16, CW)

    def combine(d):
        p_wait(osend, oret, o_ss, o_rs, d)
        rows = oret[d].reshape(512, CW)
        part = f32dot(mix_hi[d], rows) + f32dot(mix_lo[d], rows)
        if d:
            ysend[d] = part.astype(BF16).reshape(4, 64, CW)
            z_copy(ysend, yback, y_ss, y_rs, d, -1).start()
        else:
            yback[0] = part.astype(BF16).reshape(4, 64, CW)

    dispatch(0, zsend)
    dispatch(1, zrecv)
    dispatch(3, zrecv)
    gate_load.wait()
    up_load.wait()
    down_load.wait()
    expert(0)
    dispatch(2, zrecv)
    for d in OFFSETS:
        expert(d)
        p_start(osend, oret, o_ss, o_rs, d)
    p_start(osend, oret, o_ss, o_rs, 0)
    for d in OFFSETS:
        combine(d)
    combine(0)
    for d in OFFSETS:
        z_copy(ysend, yback, y_ss, y_rs, d, -1).wait_recv()
    for q in range(4):
        cols = slice(q * CW, (q + 1) * CW)
        moe = f32dot(from_plane[...], jnp.concatenate([yback[d, q] for d in range(4)], axis=0))
        out_ref[:, cols] = (hidden_ref[:, cols].astype(F32) + moe).astype(BF16)

    for d in range(1, 4):
        z_copy(msend, mrecv, m_ss, m_rs, d).wait_send()
        z_copy(zsend, zrecv, z_ss, z_rs, d).wait_send()
        z_copy(ysend, yback, y_ss, y_rs, d, -1).wait_send()

    def sent(i, _):
        for d in range(4):
            p_copy(psend, precv, p_ss, p_rs, i, d).wait_send()
            p_copy(osend, oret, o_ss, o_rs, i, d).wait_send()
        return 0

    lax.fori_loop(1, 32, sent, 0)


def layer(*arrays):
    vmem = pl.BlockSpec(memory_space=pltpu.VMEM)
    smem = pl.BlockSpec(memory_space=pltpu.SMEM)
    hbm = pl.BlockSpec(memory_space=pltpu.HBM)
    dma = pltpu.SemaphoreType.DMA
    return pl.pallas_call(
        layer_kernel,
        out_shape=jax.ShapeDtypeStruct((128, 2048), BF16),
        in_specs=[hbm] * 3 + [vmem, smem, hbm, vmem, hbm, vmem, vmem, vmem] + [hbm] * 3,
        out_specs=vmem,
        scratch_shapes=[pltpu.VMEM((128, 1024), BF16)] * 3
        + [pltpu.VMEM((128, 2048), BF16), pltpu.VMEM((1024, 2048), BF16), pltpu.VMEM((128, 2048), BF16)]
        + [pltpu.VMEM((16, 208, 128), BF16)] * 2
        + [pltpu.VMEM((16, 64, 128), BF16)] * 2
        + [pltpu.VMEM((2048, 128), BF16)] * 3
        + [pltpu.VMEM((8, 2048), F32), pltpu.VMEM((128, 1024), BF16)]
        + [pltpu.VMEM((256, 128), BF16), pltpu.VMEM((128, 256), BF16), pltpu.VMEM((4, 512, 256), BF16)]
        + [pltpu.VMEM((4, 256, 512), BF16)] * 2
        + [pltpu.VMEM((512, 512), BF16)] * 2
        + [pltpu.VMEM((4, 64, 128), BF16)] * 2
        + [pltpu.VMEM((4, 4, 64, CW), BF16)] * 2
        + [pltpu.VMEM((4, 32, 16, CW), BF16)] * 4
        + [pltpu.VMEM((4, 4, 64, CW), BF16)] * 2
        + [pltpu.VMEM((2048, 1024), BF16)] * 2
        + [pltpu.VMEM((1024, 2048), BF16)]
        + [pltpu.VMEM((128, 2048), BF16), pltpu.VMEM((128, 1024), BF16), pltpu.VMEM((4, 128, CW), BF16)]
        + [dma((16,))] * 4
        + [dma((4,))] * 2
        + [dma((4,))] * 2
        + [dma((4, 32))] * 4
        + [dma((4,))] * 2
        + [dma((8,))],
        compiler_params=pltpu.CompilerParams(
            collective_id=1, has_side_effects=True, vmem_limit_bytes=60 * 2**20
        ),
    )(*arrays)


def on_device(
    stream,
    queries,
    keys_in,
    values_in,
    key_shift,
    head_shift,
    mix_gain,
    out_weight,
    post_gain,
    route,
    route_weight,
    w_gate,
    w_up,
    w_down,
):
    result = layer(
        queries[0], keys_in[0], values_in[0], key_shift[0].T, head_shift, stream[0], mix_gain[None],
        out_weight, post_gain[None], route[0].T, route_weight[0].T, w_gate[0], w_up[0], w_down[0],
    )
    return result[None]


def solution(mesh):
    placed = (
        P("dp", SP, None),
        P("dp", SP, None),
        P("dp", SP, None),
        P("dp", SP, None),
        P("dp", SP, None),
        P(),
        P(),
        P(),
        P(),
        P("dp", SP, None),
        P("dp", SP, None),
        P(SP_DP, None, None),
        P(SP_DP, None, None),
        P(SP_DP, None, None),
    )
    return jax.shard_map(
        on_device, mesh=mesh, in_specs=placed, out_specs=P("dp", SP, None), check_vma=False
    )
```

```python
import jax
import jax.numpy as jnp
from jax import lax
from jax.sharding import PartitionSpec as P
from jax.experimental import pallas as pl
from jax.experimental.pallas import tpu as pltpu

SP = "sp"
SP_DP = ("sp", "dp")
norm_eps = 1e-05
STEP = 11
CW = 512
OFFSETS = (1, 3, 2)
ROUTES = (
    (1, 1), (3, 3), (1, 3), (3, 1), (0, 1), (1, 0), (0, 3), (3, 0),
    (0, 2), (2, 0), (2, 2), (1, 2), (2, 1), (3, 2), (2, 3),
)
WIDE = 512

LOG2E = 1.4426950408889634
KB = 256
QB = 512
NT = (((1,), (1,)), ((), ()))
BF16 = jnp.bfloat16
F32 = jnp.float32


def picker(rows, cols, fn):
    r = lax.broadcasted_iota(jnp.int32, (rows, cols), 0)
    c = lax.broadcasted_iota(jnp.int32, (rows, cols), 1)
    return jnp.where(fn(r, c), 1.0, 0.0).astype(BF16)


def f32dot(a, b):
    return jnp.dot(a, b, preferred_element_type=F32)


def half_pickers():
    low_low = picker(128, 128, lambda r, c: (r == c) & (c < 64))
    low_high = picker(128, 128, lambda r, c: r == c - 64)
    high_low = picker(128, 128, lambda r, c: r == c + 64)
    high_high = picker(128, 128, lambda r, c: (r == c) & (c >= 64))
    return (low_low, low_high), (high_low, high_high)


def row_iota(rows, cols):
    return lax.broadcasted_iota(jnp.int32, (rows, cols), 0)


def col_iota(rows, cols):
    return lax.broadcasted_iota(jnp.int32, (rows, cols), 1)


def as_whole(x):
    return x.astype(jnp.int32)


def layer_kernel(
    q_hbm, k_hbm, v_hbm, shift_ref, head_shift_ref, stream_hbm, mix_ref, w_hbm, post_ref,
    route_ref, weight_ref, gate_hbm, up_hbm, down_hbm,
    out_ref,
    q_ref, k_ref, v_ref, stream_ref, w_vmem, hidden_ref,
    sendbuf, recvbuf, attsend, attrecv, qs, kk, vv, off, normed,
    to_plane, from_plane, to_experts, mix_hi, mix_lo, spread, gather,
    msend, mrecv, zsend, zrecv, psend, precv, osend, oret, ysend, yback,
    gate_w, up_w, down_w, xs, inner, outs,
    send_sem, recv_sem, asend_sem, arecv_sem,
    m_ss, m_rs, z_ss, z_rs, p_ss, p_rs, o_ss, o_rs, y_ss, y_rs, load_sem,
):
    me, dp = lax.axis_index("sp"), lax.axis_index("dp")
    z, y = me // 4, lax.rem(me, 4)
    place = y * 8 + dp
    mesh_id = pl.DeviceIdType.MESH

    def on_z(at):
        return {"sp": at * 4 + y}

    def in_plane(p):
        return {"sp": z * 4 + p // 8, "dp": lax.rem(p, 8)}

    def plane_peer(i):
        o = lax.rem(i * STEP, 32)
        py = lax.rem(place // 8 + o // 8, 4)
        px = lax.rem(lax.rem(place, 8) // 2 + lax.rem(o, 8) // 2, 4)
        pc = lax.rem(place + o, 2)
        return py * 8 + px * 2 + pc

    turn = 1 - 2 * lax.rem(dp, 2)

    def sp_peer(i, way):
        dz, dy = ROUTES[i]
        to_z = lax.rem(z + 4 + way * turn * dz, 4)
        return to_z * 4 + lax.rem(y + 4 + way * turn * dy, 4)

    barrier = pltpu.get_barrier_semaphore()

    def greet_sp(d, _):
        pl.semaphore_signal(
            barrier, inc=1, device_id={"sp": lax.rem(me + d, 16)}, device_id_type=mesh_id
        )
        return 0

    def greet_plane(i, _):
        pl.semaphore_signal(barrier, inc=1, device_id=in_plane(plane_peer(i)), device_id_type=mesh_id)
        return 0

    lax.fori_loop(1, 16, greet_sp, 0)
    lax.fori_loop(1, 32, greet_plane, 0)
    loads = [
        pltpu.make_async_copy(a, b, load_sem.at[i])
        for i, (a, b) in enumerate((
            (q_hbm, q_ref), (k_hbm, k_ref), (v_hbm, v_ref), (stream_hbm, stream_ref),
            (w_hbm, w_vmem), (gate_hbm, gate_w), (up_hbm, up_w), (down_hbm, down_w),
        ))
    ]
    for c in loads:
        c.start()
    q_load, k_load, v_load, stream_load, w_load, gate_load, up_load, down_load = loads

    pickers = half_pickers()
    shifts = shift_ref[...].astype(F32)
    q_load.wait()
    k_load.wait()
    v_load.wait()
    for h in range(16):
        tile = slice((h // 2) * 128, (h // 2 + 1) * 128)
        first, second = pickers[h % 2]
        sendbuf[h, 0:128, :] = (f32dot(q_ref[:, tile], first) + f32dot(k_ref[:, tile], second)).astype(BF16)
        sendbuf[h, 128:192, :] = (
            f32dot(v_ref[0:64, tile], first) + f32dot(v_ref[64:128, tile], second)
        ).astype(BF16)
        sendbuf[h, 192:208, :] = jnp.broadcast_to(shifts[h:h + 1, :], (16, 128)).astype(BF16)

    pl.semaphore_wait(barrier, 46)

    def z_copy(src, dst, ss, rs, d, way=1):
        return pltpu.make_async_remote_copy(
            src_ref=src.at[d],
            dst_ref=dst.at[d],
            send_sem=ss.at[d],
            recv_sem=rs.at[d],
            device_id=on_z(lax.rem(z + 4 + way * d, 4)),
            device_id_type=mesh_id,
        )

    def p_copy(src, dst, ss, rs, i, d):
        to = plane_peer(i)
        return pltpu.make_async_remote_copy(
            src_ref=src.at[d, to],
            dst_ref=dst.at[d, place],
            send_sem=ss.at[d, i],
            recv_sem=rs.at[d, i],
            device_id=in_plane(to),
            device_id_type=mesh_id,
        )

    def p_start(src, dst, ss, rs, d):
        def one(i, _):
            p_copy(src, dst, ss, rs, i, d).start()
            return 0

        lax.fori_loop(1, 32, one, 0)
        dst[d, place] = src[d, place]

    def p_wait(src, dst, ss, rs, d):
        def one(i, _):
            p_copy(src, dst, ss, rs, i, d).wait_recv()
            return 0

        lax.fori_loop(1, 32, one, 0)

    def outgoing(i):
        to = sp_peer(i, 1)
        return pltpu.make_async_remote_copy(
            src_ref=sendbuf.at[to],
            dst_ref=recvbuf.at[me],
            send_sem=send_sem.at[i],
            recv_sem=recv_sem.at[i],
            device_id={"sp": to},
            device_id_type=mesh_id,
        )

    for i in range(15):
        outgoing(i).start()
    recvbuf[me] = sendbuf[me]

    lanes = col_iota(128, 128)
    w_row = weight_ref[...]
    w_hi = w_row.astype(BF16).astype(F32)
    facts = jnp.concatenate(
        [route_ref[...].astype(F32), w_hi, w_row - w_hi, jnp.zeros((10, 128), F32)], axis=0
    ).astype(BF16)
    whole_eye = picker(128, 128, lambda r, c: r == c)
    by_token = lax.dot_general(whole_eye, facts, NT, preferred_element_type=F32)
    first, second = as_whole(by_token[:, 0:1]), as_whole(by_token[:, 1:2])
    in_first = jnp.where(lanes == first, 1.0, 0.0)
    in_second = jnp.where(lanes == second, 1.0, 0.0)
    before = picker(128, 128, lambda r, c: c < r)
    named = f32dot(before, (in_first + in_second).astype(BF16))
    rank_first = jnp.sum(in_first * named, axis=1, keepdims=True)
    rank_second = jnp.sum(in_second * named, axis=1, keepdims=True)
    group = (lax.shift_right_logical(first, 5) - z) & 3
    in_group = jnp.where(lanes == group, 1.0, 0.0)
    within = jnp.sum(in_group * f32dot(before, in_group.astype(BF16)), axis=1, keepdims=True)
    fields = (
        ((first & 31) + 1).astype(F32), rank_first, ((second & 31) + 1).astype(F32), rank_second,
        by_token[:, 2:3], by_token[:, 4:5], by_token[:, 3:4], by_token[:, 5:6], group.astype(F32), within,
    )
    table = jnp.zeros((128, 128), F32)
    for i, field in enumerate(fields):
        table = jnp.where(lanes == i, field, table)
    table = table.astype(BF16)
    eye = picker(16, 128, lambda r, c: r == c)
    by_lane = lax.dot_general(eye, table, NT, preferred_element_type=F32)
    goes_to = as_whole(by_lane[8:9] * 64.0 + by_lane[9:10])
    to_plane[...] = jnp.where(row_iota(256, 128) == goes_to, 1.0, 0.0).astype(BF16)
    from_plane[...] = jnp.where(
        col_iota(128, 256) == group * 64 + as_whole(within), 1.0, 0.0
    ).astype(BF16)
    msend[...] = f32dot(to_plane[...], table).astype(BF16).reshape(4, 64, 128)

    for d in range(1, 4):
        z_copy(msend, mrecv, m_ss, m_rs, d).start()
    mrecv[0] = msend[0]

    for d in range(1, 4):
        z_copy(msend, mrecv, m_ss, m_rs, d).wait_recv()
    def slots(p, rank, quarter):
        at = (as_whole(p) - 1) * 16 + quarter * 4 + as_whole(rank)
        return jnp.where(p > 0.5, at, -1)

    lane_quarter = lax.shift_right_logical(col_iota(1, 256), 6)
    row_quarter = lax.shift_right_logical(row_iota(256, 1), 6)
    for d in range(4):
        got = jnp.concatenate([mrecv[d]] * 4, axis=0)
        by_lane = lax.dot_general(eye, got, NT, preferred_element_type=F32)
        by_row = got.astype(F32)
        slot0 = slots(by_lane[0:1], by_lane[1:2], lane_quarter)
        slot1 = slots(by_lane[2:3], by_lane[3:4], lane_quarter)
        at = row_iota(512, 256)
        to_experts[d] = jnp.where((at == slot0) | (at == slot1), 1.0, 0.0).astype(BF16)
        slot0 = slots(by_row[:, 0:1], by_row[:, 1:2], row_quarter)
        slot1 = slots(by_row[:, 2:3], by_row[:, 3:4], row_quarter)
        at = col_iota(256, 512)
        is0, is1 = at == slot0, at == slot1
        mix_hi[d] = jnp.where(is0, by_row[:, 4:5], jnp.where(is1, by_row[:, 6:7], 0.0)).astype(BF16)
        mix_lo[d] = jnp.where(is0, by_row[:, 5:6], jnp.where(is1, by_row[:, 7:8], 0.0)).astype(BF16)

    def message_row(stacked):
        return (stacked & 127) // 4 * 16 + lax.shift_right_logical(stacked, 7) * 4 + (stacked & 3)

    spread[...] = jnp.where(row_iota(512, 512) == message_row(col_iota(1, 512)), 1.0, 0.0).astype(BF16)
    gather[...] = jnp.where(col_iota(512, 512) == message_row(row_iota(512, 1)), 1.0, 0.0).astype(BF16)

    both_low = picker(128, 128, lambda r, c: r == c % 64)
    both_high = picker(128, 128, lambda r, c: r == c % 64 + 64)
    lane = col_iota(128, 128)
    hs = head_shift_ref[me]

    def unpack(j):
        at = pl.multiple_of(j * 128, 128)
        rows = pl.ds(at, 128)
        qk = recvbuf[j, 0:128, :]
        q2 = f32dot(qk, both_low) * (LOG2E / 8.0)
        hi = q2.astype(BF16).astype(F32)
        qs[rows, :] = jnp.where(lane < 64, hi, q2 - hi).astype(BF16)
        kk[rows, :] = f32dot(qk, both_high).astype(BF16)
        vm = recvbuf[j, 128:192, :]
        vv[pl.ds(at, 64), :] = f32dot(vm, both_low).astype(BF16)
        vv[pl.ds(pl.multiple_of(at + 64, 64), 64), :] = f32dot(vm, both_high).astype(BF16)
        off[0:1, rows] = (recvbuf[j, 192:208, :].astype(F32)[0:1] + hs) * LOG2E

    unpack(me)
    for i in range(15):
        outgoing(i).wait_recv()
        unpack(sp_peer(i, -1))

    tri = picker(KB, KB, lambda r, c: r >= c)
    lane64 = lax.broadcasted_iota(jnp.int32, (64, 128), 1) < 64

    def reply(j):
        return pltpu.make_async_remote_copy(
            src_ref=attsend.at[j],
            dst_ref=attrecv.at[me],
            send_sem=asend_sem.at[j],
            recv_sem=arecv_sem.at[me],
            device_id={"sp": j},
            device_id_type=pl.DeviceIdType.MESH,
        )

    for qi in range(2048 // QB):
        r0 = qi * QB
        carry = jnp.zeros((QB, 1), F32)
        acc = jnp.zeros((QB, 128), F32)
        for ki in range((r0 + QB) // KB - 1, -1, -1):
            k0 = ki * KB
            logit = lax.dot_general(qs[r0:r0 + QB, :], kk[k0:k0 + KB, :], NT, preferred_element_type=F32)
            logit = logit + off[0:1, k0:k0 + KB]
            sp = jnp.maximum(logit, jnp.log2(1.0 + jnp.exp2(jnp.minimum(logit, 100.0))))
            masked = k0 >= r0
            if masked:
                r = lax.broadcasted_iota(jnp.int32, (QB, KB), 0)
                c = lax.broadcasted_iota(jnp.int32, (QB, KB), 1)
                earlier = c - r < r0 - k0
                sp = jnp.where(earlier, sp, 0.0)
            hi = sp.astype(BF16)
            lo = (sp - hi.astype(F32)).astype(BF16)
            s = f32dot(hi, tri) + f32dot(lo, tri)
            w = jnp.exp2((logit - s) - carry)
            if masked:
                w = jnp.where(earlier, w, 0.0)
            acc = acc + f32dot(w.astype(BF16), vv[k0:k0 + KB, :])
            carry = carry + s[:, 0:1]
        for part in range(QB // 128):
            j = r0 // 128 + part
            at = part * 128
            attsend[j] = jnp.where(lane64, acc[at:at + 64], acc[at + 64:at + 128]).astype(BF16)

            @pl.when(me != j)
            def _():
                reply(j).start()

            @pl.when(me == j)
            def _():
                attrecv[j] = attsend[j]

    for j in range(16):
        @pl.when(me != j)
        def _():
            reply(j).wait_send()
            pltpu.make_async_remote_copy(
                src_ref=attsend.at[j],
                dst_ref=attrecv.at[j],
                send_sem=asend_sem.at[j],
                recv_sem=arecv_sem.at[j],
                device_id={"sp": j},
                device_id_type=pl.DeviceIdType.MESH,
            ).wait_recv()

    (low_low, low_high), (high_low, high_high) = pickers
    squares = jnp.zeros((128, 1), F32)
    tiles = []
    for p in range(8):
        even, odd = attrecv[2 * p], attrecv[2 * p + 1]
        low = f32dot(even, low_low) + f32dot(odd, low_high)
        high = f32dot(even, high_low) + f32dot(odd, high_high)
        tile = jnp.concatenate([low, high], axis=0)
        squares = squares + jnp.sum(tile * tile, axis=1, keepdims=True)
        tiles.append(tile)
    inv = lax.rsqrt(squares * (1.0 / 1024.0) + norm_eps)
    for p in range(8):
        cols = slice(p * 128, (p + 1) * 128)
        normed[:, cols] = (tiles[p] * inv * mix_ref[:, cols]).astype(BF16)
    w_load.wait()
    stream_load.wait()
    totals = jnp.zeros((128, 1), F32)
    sums = []
    for n in range(8):
        cols = slice(n * 256, (n + 1) * 256)
        summed = stream_ref[:, cols].astype(F32) + f32dot(normed[...], w_vmem[:, cols])
        totals = totals + jnp.sum(summed * summed, axis=1, keepdims=True)
        sums.append(summed)
    inv = lax.rsqrt(totals * (1.0 / 2048.0) + norm_eps)
    for n in range(8):
        cols = slice(n * 256, (n + 1) * 256)
        hidden_ref[:, cols] = (sums[n] * inv * post_ref[:, cols]).astype(BF16)

    for q in range(4):
        rows = f32dot(to_plane[...], hidden_ref[:, q * CW:(q + 1) * CW]).astype(BF16)
        for d in range(4):
            zsend[d, q] = rows[d * 64:(d + 1) * 64]
    for d in OFFSETS:
        z_copy(zsend, zrecv, z_ss, z_rs, d).start()

    def dispatch(d, source):
        if d:
            z_copy(zsend, zrecv, z_ss, z_rs, d).wait_recv()
        psend[d] = f32dot(to_experts[d], source[d].reshape(256, CW)).astype(BF16).reshape(32, 16, CW)
        p_start(psend, precv, p_ss, p_rs, d)

    def expert(d):
        p_wait(psend, precv, p_ss, p_rs, d)
        stacked = f32dot(gather[...], precv[d].reshape(512, CW)).astype(BF16)
        for q in range(4):
            xs[:, q * CW:(q + 1) * CW] = stacked[q * 128:(q + 1) * 128]

        def first_half(n, _):
            cols = pl.ds(pl.multiple_of(n * WIDE, WIDE), WIDE)
            g = f32dot(xs[...], gate_w[:, cols])
            u = f32dot(xs[...], up_w[:, cols])
            inner[:, cols] = (g / (1.0 + jnp.exp(-g)) * u).astype(BF16)
            return 0

        lax.fori_loop(0, 1024 // WIDE, first_half, 0)

        def second_half(q, _):
            cols = pl.ds(pl.multiple_of(q * CW, CW), CW)
            outs[q] = f32dot(inner[...], down_w[:, cols]).astype(BF16)
            return 0

        lax.fori_loop(0, 4, second_half, 0)
        osend[d] = f32dot(spread[...], outs[...].reshape(512, CW)).astype(BF16).reshape(32, 16, CW)

    def combine(d):
        p_wait(osend, oret, o_ss, o_rs, d)
        rows = oret[d].reshape(512, CW)
        part = f32dot(mix_hi[d], rows) + f32dot(mix_lo[d], rows)
        if d:
            ysend[d] = part.astype(BF16).reshape(4, 64, CW)
            z_copy(ysend, yback, y_ss, y_rs, d, -1).start()
        else:
            yback[0] = part.astype(BF16).reshape(4, 64, CW)

    dispatch(0, zsend)
    dispatch(1, zrecv)
    dispatch(3, zrecv)
    gate_load.wait()
    up_load.wait()
    down_load.wait()
    expert(0)
    dispatch(2, zrecv)
    for d in OFFSETS:
        expert(d)
        p_start(osend, oret, o_ss, o_rs, d)
    p_start(osend, oret, o_ss, o_rs, 0)
    for d in OFFSETS:
        combine(d)
    combine(0)
    for d in OFFSETS:
        z_copy(ysend, yback, y_ss, y_rs, d, -1).wait_recv()
    for q in range(4):
        cols = slice(q * CW, (q + 1) * CW)
        moe = f32dot(from_plane[...], jnp.concatenate([yback[d, q] for d in range(4)], axis=0))
        out_ref[:, cols] = (hidden_ref[:, cols].astype(F32) + moe).astype(BF16)

    for i in range(15):
        outgoing(i).wait_send()
    for d in range(1, 4):
        z_copy(msend, mrecv, m_ss, m_rs, d).wait_send()
        z_copy(zsend, zrecv, z_ss, z_rs, d).wait_send()
        z_copy(ysend, yback, y_ss, y_rs, d, -1).wait_send()

    def sent(i, _):
        for d in range(4):
            p_copy(psend, precv, p_ss, p_rs, i, d).wait_send()
            p_copy(osend, oret, o_ss, o_rs, i, d).wait_send()
        return 0

    lax.fori_loop(1, 32, sent, 0)


def layer(*arrays):
    vmem = pl.BlockSpec(memory_space=pltpu.VMEM)
    smem = pl.BlockSpec(memory_space=pltpu.SMEM)
    hbm = pl.BlockSpec(memory_space=pltpu.HBM)
    dma = pltpu.SemaphoreType.DMA
    return pl.pallas_call(
        layer_kernel,
        out_shape=pltpu.VMEM((128, 2048), BF16),
        in_specs=[hbm] * 3 + [vmem, smem, hbm, vmem, hbm, vmem, vmem, vmem] + [hbm] * 3,
        out_specs=vmem,
        scratch_shapes=[pltpu.VMEM((128, 1024), BF16)] * 3
        + [pltpu.VMEM((128, 2048), BF16), pltpu.VMEM((1024, 2048), BF16), pltpu.VMEM((128, 2048), BF16)]
        + [pltpu.VMEM((16, 208, 128), BF16)] * 2
        + [pltpu.VMEM((16, 64, 128), BF16)] * 2
        + [pltpu.VMEM((2048, 128), BF16)] * 3
        + [pltpu.VMEM((8, 2048), F32), pltpu.VMEM((128, 1024), BF16)]
        + [pltpu.VMEM((256, 128), BF16), pltpu.VMEM((128, 256), BF16), pltpu.VMEM((4, 512, 256), BF16)]
        + [pltpu.VMEM((4, 256, 512), BF16)] * 2
        + [pltpu.VMEM((512, 512), BF16)] * 2
        + [pltpu.VMEM((4, 64, 128), BF16)] * 2
        + [pltpu.VMEM((4, 4, 64, CW), BF16)] * 2
        + [pltpu.VMEM((4, 32, 16, CW), BF16)] * 4
        + [pltpu.VMEM((4, 4, 64, CW), BF16)] * 2
        + [pltpu.VMEM((2048, 1024), BF16)] * 2
        + [pltpu.VMEM((1024, 2048), BF16)]
        + [pltpu.VMEM((128, 2048), BF16), pltpu.VMEM((128, 1024), BF16), pltpu.VMEM((4, 128, CW), BF16)]
        + [dma((16,))] * 4
        + [dma((4,))] * 2
        + [dma((4,))] * 2
        + [dma((4, 32))] * 4
        + [dma((4,))] * 2
        + [dma((8,))],
        compiler_params=pltpu.CompilerParams(
            collective_id=1, has_side_effects=True, vmem_limit_bytes=60 * 2**20
        ),
    )(*arrays)


def on_device(
    stream,
    queries,
    keys_in,
    values_in,
    key_shift,
    head_shift,
    mix_gain,
    out_weight,
    post_gain,
    route,
    route_weight,
    w_gate,
    w_up,
    w_down,
):
    result = layer(
        queries[0], keys_in[0], values_in[0], key_shift[0].T, head_shift, stream[0], mix_gain[None],
        out_weight, post_gain[None], route[0].T, route_weight[0].T, w_gate[0], w_up[0], w_down[0],
    )
    return result[None]


def solution(mesh):
    placed = (
        P("dp", SP, None),
        P("dp", SP, None),
        P("dp", SP, None),
        P("dp", SP, None),
        P("dp", SP, None),
        P(),
        P(),
        P(),
        P(),
        P("dp", SP, None),
        P("dp", SP, None),
        P(SP_DP, None, None),
        P(SP_DP, None, None),
        P(SP_DP, None, None),
    )
    return jax.shard_map(
        on_device, mesh=mesh, in_specs=placed, out_specs=P("dp", SP, None), check_vma=False
    )
```

```python
import jax
import jax.numpy as jnp
from jax import lax
from jax.sharding import PartitionSpec as P
from jax.experimental import pallas as pl
from jax.experimental.pallas import tpu as pltpu

SP = "sp"
SP_DP = ("sp", "dp")
norm_eps = 1e-05
TURNS = (
    ((1, 1), (3, 3)), ((1, 3), (3, 1)), ((0, 1), (1, 0), (0, 3), (3, 0)),
    ((0, 2), (2, 0)), ((2, 2),), ((1, 2), (2, 1), (3, 2), (2, 3)),
)
PLANE = tuple(dy * 8 + dx * 2 + dc for turn in TURNS for dc in (0, 1) for dy, dx in turn) + (1,)
CW = 512
OFFSETS = (1, 3, 2)
ROUTES = (
    (1, 1), (3, 3), (1, 3), (3, 1), (0, 1), (1, 0), (0, 3), (3, 0),
    (0, 2), (2, 0), (2, 2), (1, 2), (2, 1), (3, 2), (2, 3),
)
WIDE = 512

LOG2E = 1.4426950408889634
KB = 256
QB = 512
NT = (((1,), (1,)), ((), ()))
BF16 = jnp.bfloat16
F32 = jnp.float32


def picker(rows, cols, fn):
    r = lax.broadcasted_iota(jnp.int32, (rows, cols), 0)
    c = lax.broadcasted_iota(jnp.int32, (rows, cols), 1)
    return jnp.where(fn(r, c), 1.0, 0.0).astype(BF16)


def f32dot(a, b):
    return jnp.dot(a, b, preferred_element_type=F32)


def half_pickers():
    low_low = picker(128, 128, lambda r, c: (r == c) & (c < 64))
    low_high = picker(128, 128, lambda r, c: r == c - 64)
    high_low = picker(128, 128, lambda r, c: r == c + 64)
    high_high = picker(128, 128, lambda r, c: (r == c) & (c >= 64))
    return (low_low, low_high), (high_low, high_high)


def row_iota(rows, cols):
    return lax.broadcasted_iota(jnp.int32, (rows, cols), 0)


def col_iota(rows, cols):
    return lax.broadcasted_iota(jnp.int32, (rows, cols), 1)


def as_whole(x):
    return x.astype(jnp.int32)


def layer_kernel(
    q_hbm, k_hbm, v_hbm, shift_ref, head_shift_ref, stream_hbm, mix_ref, w_hbm, post_ref,
    route_ref, weight_ref, gate_hbm, up_hbm, down_hbm,
    out_ref,
    q_ref, k_ref, v_ref, stream_ref, w_vmem, hidden_ref,
    sendbuf, recvbuf, attsend, attrecv, qs, kk, vv, off, normed,
    to_plane, from_plane, to_experts, mix_hi, mix_lo, spread, gather,
    msend, mrecv, zsend, zrecv, psend, precv, osend, oret, ysend, yback,
    gate_w, up_w, down_w, xs, inner, outs,
    send_sem, recv_sem, asend_sem, arecv_sem,
    m_ss, m_rs, z_ss, z_rs, p_ss, p_rs, o_ss, o_rs, y_ss, y_rs, load_sem,
):
    me, dp = lax.axis_index("sp"), lax.axis_index("dp")
    z, y = me // 4, lax.rem(me, 4)
    place = y * 8 + dp
    mesh_id = pl.DeviceIdType.MESH

    def on_z(at):
        return {"sp": at * 4 + y}

    def in_plane(p):
        return {"sp": z * 4 + p // 8, "dp": lax.rem(p, 8)}

    def plane_peer(o):
        py = lax.rem(place // 8 + o // 8, 4)
        px = lax.rem(lax.rem(place, 8) // 2 + o % 8 // 2, 4)
        pc = lax.rem(place + o, 2)
        return py * 8 + px * 2 + pc

    turn = 1 - 2 * lax.rem(dp, 2)

    def sp_peer(i, way):
        dz, dy = ROUTES[i]
        to_z = lax.rem(z + 4 + way * turn * dz, 4)
        return to_z * 4 + lax.rem(y + 4 + way * turn * dy, 4)

    barrier = pltpu.get_barrier_semaphore()

    def greet_sp(d, _):
        pl.semaphore_signal(
            barrier, inc=1, device_id={"sp": lax.rem(me + d, 16)}, device_id_type=mesh_id
        )
        return 0

    def greet_plane(i, _):
        pl.semaphore_signal(barrier, inc=1, device_id=in_plane(plane_peer(i)), device_id_type=mesh_id)
        return 0

    lax.fori_loop(1, 16, greet_sp, 0)
    lax.fori_loop(1, 32, greet_plane, 0)
    loads = [
        pltpu.make_async_copy(a, b, load_sem.at[i])
        for i, (a, b) in enumerate((
            (q_hbm, q_ref), (k_hbm, k_ref), (v_hbm, v_ref), (stream_hbm, stream_ref),
            (w_hbm, w_vmem), (gate_hbm, gate_w), (up_hbm, up_w), (down_hbm, down_w),
        ))
    ]
    for c in loads:
        c.start()
    q_load, k_load, v_load, stream_load, w_load, gate_load, up_load, down_load = loads

    pickers = half_pickers()
    shifts = shift_ref[...].astype(F32)
    q_load.wait()
    k_load.wait()
    v_load.wait()
    for h in range(16):
        tile = slice((h // 2) * 128, (h // 2 + 1) * 128)
        first, second = pickers[h % 2]
        sendbuf[h, 0:128, :] = (f32dot(q_ref[:, tile], first) + f32dot(k_ref[:, tile], second)).astype(BF16)
        sendbuf[h, 128:192, :] = (
            f32dot(v_ref[0:64, tile], first) + f32dot(v_ref[64:128, tile], second)
        ).astype(BF16)
        sendbuf[h, 192:208, :] = jnp.broadcast_to(shifts[h:h + 1, :], (16, 128)).astype(BF16)

    pl.semaphore_wait(barrier, 46)

    def z_copy(src, dst, ss, rs, d, way=1):
        return pltpu.make_async_remote_copy(
            src_ref=src.at[d],
            dst_ref=dst.at[d],
            send_sem=ss.at[d],
            recv_sem=rs.at[d],
            device_id=on_z(lax.rem(z + 4 + way * d, 4)),
            device_id_type=mesh_id,
        )

    def p_copy(src, dst, ss, rs, i, d):
        to = plane_peer(i)
        return pltpu.make_async_remote_copy(
            src_ref=src.at[d, to],
            dst_ref=dst.at[d, place],
            send_sem=ss.at[d, i],
            recv_sem=rs.at[d, i],
            device_id=in_plane(to),
            device_id_type=mesh_id,
        )

    def p_start(src, dst, ss, rs, d):
        for o in PLANE:
            p_copy(src, dst, ss, rs, o, d).start()
        dst[d, place] = src[d, place]

    def p_wait(src, dst, ss, rs, d):
        def one(i, _):
            p_copy(src, dst, ss, rs, i, d).wait_recv()
            return 0

        lax.fori_loop(1, 32, one, 0)

    def outgoing(i):
        to = sp_peer(i, 1)
        return pltpu.make_async_remote_copy(
            src_ref=sendbuf.at[to],
            dst_ref=recvbuf.at[me],
            send_sem=send_sem.at[i],
            recv_sem=recv_sem.at[i],
            device_id={"sp": to},
            device_id_type=mesh_id,
        )

    for i in range(15):
        outgoing(i).start()
    recvbuf[me] = sendbuf[me]

    lanes = col_iota(128, 128)
    w_row = weight_ref[...]
    w_hi = w_row.astype(BF16).astype(F32)
    facts = jnp.concatenate(
        [route_ref[...].astype(F32), w_hi, w_row - w_hi, jnp.zeros((10, 128), F32)], axis=0
    ).astype(BF16)
    whole_eye = picker(128, 128, lambda r, c: r == c)
    by_token = lax.dot_general(whole_eye, facts, NT, preferred_element_type=F32)
    first, second = as_whole(by_token[:, 0:1]), as_whole(by_token[:, 1:2])
    in_first = jnp.where(lanes == first, 1.0, 0.0)
    in_second = jnp.where(lanes == second, 1.0, 0.0)
    before = picker(128, 128, lambda r, c: c < r)
    named = f32dot(before, (in_first + in_second).astype(BF16))
    rank_first = jnp.sum(in_first * named, axis=1, keepdims=True)
    rank_second = jnp.sum(in_second * named, axis=1, keepdims=True)
    group = (lax.shift_right_logical(first, 5) - z) & 3
    in_group = jnp.where(lanes == group, 1.0, 0.0)
    within = jnp.sum(in_group * f32dot(before, in_group.astype(BF16)), axis=1, keepdims=True)
    fields = (
        ((first & 31) + 1).astype(F32), rank_first, ((second & 31) + 1).astype(F32), rank_second,
        by_token[:, 2:3], by_token[:, 4:5], by_token[:, 3:4], by_token[:, 5:6], group.astype(F32), within,
    )
    table = jnp.zeros((128, 128), F32)
    for i, field in enumerate(fields):
        table = jnp.where(lanes == i, field, table)
    table = table.astype(BF16)
    eye = picker(16, 128, lambda r, c: r == c)
    by_lane = lax.dot_general(eye, table, NT, preferred_element_type=F32)
    goes_to = as_whole(by_lane[8:9] * 64.0 + by_lane[9:10])
    to_plane[...] = jnp.where(row_iota(256, 128) == goes_to, 1.0, 0.0).astype(BF16)
    from_plane[...] = jnp.where(
        col_iota(128, 256) == group * 64 + as_whole(within), 1.0, 0.0
    ).astype(BF16)
    msend[...] = f32dot(to_plane[...], table).astype(BF16).reshape(4, 64, 128)

    for d in range(1, 4):
        z_copy(msend, mrecv, m_ss, m_rs, d).start()
    mrecv[0] = msend[0]

    for d in range(1, 4):
        z_copy(msend, mrecv, m_ss, m_rs, d).wait_recv()
    def slots(p, rank, quarter):
        at = (as_whole(p) - 1) * 16 + quarter * 4 + as_whole(rank)
        return jnp.where(p > 0.5, at, -1)

    lane_quarter = lax.shift_right_logical(col_iota(1, 256), 6)
    row_quarter = lax.shift_right_logical(row_iota(256, 1), 6)
    for d in range(4):
        got = jnp.concatenate([mrecv[d]] * 4, axis=0)
        by_lane = lax.dot_general(eye, got, NT, preferred_element_type=F32)
        by_row = got.astype(F32)
        slot0 = slots(by_lane[0:1], by_lane[1:2], lane_quarter)
        slot1 = slots(by_lane[2:3], by_lane[3:4], lane_quarter)
        at = row_iota(512, 256)
        to_experts[d] = jnp.where((at == slot0) | (at == slot1), 1.0, 0.0).astype(BF16)
        slot0 = slots(by_row[:, 0:1], by_row[:, 1:2], row_quarter)
        slot1 = slots(by_row[:, 2:3], by_row[:, 3:4], row_quarter)
        at = col_iota(256, 512)
        is0, is1 = at == slot0, at == slot1
        mix_hi[d] = jnp.where(is0, by_row[:, 4:5], jnp.where(is1, by_row[:, 6:7], 0.0)).astype(BF16)
        mix_lo[d] = jnp.where(is0, by_row[:, 5:6], jnp.where(is1, by_row[:, 7:8], 0.0)).astype(BF16)

    def message_row(stacked):
        return (stacked & 127) // 4 * 16 + lax.shift_right_logical(stacked, 7) * 4 + (stacked & 3)

    spread[...] = jnp.where(row_iota(512, 512) == message_row(col_iota(1, 512)), 1.0, 0.0).astype(BF16)
    gather[...] = jnp.where(col_iota(512, 512) == message_row(row_iota(512, 1)), 1.0, 0.0).astype(BF16)

    both_low = picker(128, 128, lambda r, c: r == c % 64)
    both_high = picker(128, 128, lambda r, c: r == c % 64 + 64)
    lane = col_iota(128, 128)
    hs = head_shift_ref[me]

    def unpack(j):
        at = pl.multiple_of(j * 128, 128)
        rows = pl.ds(at, 128)
        qk = recvbuf[j, 0:128, :]
        q2 = f32dot(qk, both_low) * (LOG2E / 8.0)
        hi = q2.astype(BF16).astype(F32)
        qs[rows, :] = jnp.where(lane < 64, hi, q2 - hi).astype(BF16)
        kk[rows, :] = f32dot(qk, both_high).astype(BF16)
        vm = recvbuf[j, 128:192, :]
        vv[pl.ds(at, 64), :] = f32dot(vm, both_low).astype(BF16)
        vv[pl.ds(pl.multiple_of(at + 64, 64), 64), :] = f32dot(vm, both_high).astype(BF16)
        off[0:1, rows] = (recvbuf[j, 192:208, :].astype(F32)[0:1] + hs) * LOG2E

    unpack(me)
    for i in range(15):
        outgoing(i).wait_recv()
        unpack(sp_peer(i, -1))

    tri = picker(KB, KB, lambda r, c: r >= c)
    lane64 = lax.broadcasted_iota(jnp.int32, (64, 128), 1) < 64

    def reply(j):
        return pltpu.make_async_remote_copy(
            src_ref=attsend.at[j],
            dst_ref=attrecv.at[me],
            send_sem=asend_sem.at[j],
            recv_sem=arecv_sem.at[me],
            device_id={"sp": j},
            device_id_type=pl.DeviceIdType.MESH,
        )

    for qi in range(2048 // QB):
        r0 = qi * QB
        carry = jnp.zeros((QB, 1), F32)
        acc = jnp.zeros((QB, 128), F32)
        for ki in range((r0 + QB) // KB - 1, -1, -1):
            k0 = ki * KB
            logit = lax.dot_general(qs[r0:r0 + QB, :], kk[k0:k0 + KB, :], NT, preferred_element_type=F32)
            logit = logit + off[0:1, k0:k0 + KB]
            sp = jnp.maximum(logit, jnp.log2(1.0 + jnp.exp2(jnp.minimum(logit, 100.0))))
            masked = k0 >= r0
            if masked:
                r = lax.broadcasted_iota(jnp.int32, (QB, KB), 0)
                c = lax.broadcasted_iota(jnp.int32, (QB, KB), 1)
                earlier = c - r < r0 - k0
                sp = jnp.where(earlier, sp, 0.0)
            hi = sp.astype(BF16)
            lo = (sp - hi.astype(F32)).astype(BF16)
            s = f32dot(hi, tri) + f32dot(lo, tri)
            w = jnp.exp2((logit - s) - carry)
            if masked:
                w = jnp.where(earlier, w, 0.0)
            acc = acc + f32dot(w.astype(BF16), vv[k0:k0 + KB, :])
            carry = carry + s[:, 0:1]
        for part in range(QB // 128):
            j = r0 // 128 + part
            at = part * 128
            attsend[j] = jnp.where(lane64, acc[at:at + 64], acc[at + 64:at + 128]).astype(BF16)

            @pl.when(me != j)
            def _():
                reply(j).start()

            @pl.when(me == j)
            def _():
                attrecv[j] = attsend[j]

    for j in range(16):
        @pl.when(me != j)
        def _():
            reply(j).wait_send()
            pltpu.make_async_remote_copy(
                src_ref=attsend.at[j],
                dst_ref=attrecv.at[j],
                send_sem=asend_sem.at[j],
                recv_sem=arecv_sem.at[j],
                device_id={"sp": j},
                device_id_type=pl.DeviceIdType.MESH,
            ).wait_recv()

    (low_low, low_high), (high_low, high_high) = pickers
    squares = jnp.zeros((128, 1), F32)
    tiles = []
    for p in range(8):
        even, odd = attrecv[2 * p], attrecv[2 * p + 1]
        low = f32dot(even, low_low) + f32dot(odd, low_high)
        high = f32dot(even, high_low) + f32dot(odd, high_high)
        tile = jnp.concatenate([low, high], axis=0)
        squares = squares + jnp.sum(tile * tile, axis=1, keepdims=True)
        tiles.append(tile)
    inv = lax.rsqrt(squares * (1.0 / 1024.0) + norm_eps)
    for p in range(8):
        cols = slice(p * 128, (p + 1) * 128)
        normed[:, cols] = (tiles[p] * inv * mix_ref[:, cols]).astype(BF16)
    w_load.wait()
    stream_load.wait()
    totals = jnp.zeros((128, 1), F32)
    sums = []
    for n in range(8):
        cols = slice(n * 256, (n + 1) * 256)
        summed = stream_ref[:, cols].astype(F32) + f32dot(normed[...], w_vmem[:, cols])
        totals = totals + jnp.sum(summed * summed, axis=1, keepdims=True)
        sums.append(summed)
    inv = lax.rsqrt(totals * (1.0 / 2048.0) + norm_eps)
    for n in range(8):
        cols = slice(n * 256, (n + 1) * 256)
        hidden_ref[:, cols] = (sums[n] * inv * post_ref[:, cols]).astype(BF16)

    for q in range(4):
        rows = f32dot(to_plane[...], hidden_ref[:, q * CW:(q + 1) * CW]).astype(BF16)
        for d in range(4):
            zsend[d, q] = rows[d * 64:(d + 1) * 64]
    for d in OFFSETS:
        z_copy(zsend, zrecv, z_ss, z_rs, d).start()

    def dispatch(d, source):
        if d:
            z_copy(zsend, zrecv, z_ss, z_rs, d).wait_recv()
        psend[d] = f32dot(to_experts[d], source[d].reshape(256, CW)).astype(BF16).reshape(32, 16, CW)
        p_start(psend, precv, p_ss, p_rs, d)

    def expert(d):
        p_wait(psend, precv, p_ss, p_rs, d)
        stacked = f32dot(gather[...], precv[d].reshape(512, CW)).astype(BF16)
        for q in range(4):
            xs[:, q * CW:(q + 1) * CW] = stacked[q * 128:(q + 1) * 128]

        def first_half(n, _):
            cols = pl.ds(pl.multiple_of(n * WIDE, WIDE), WIDE)
            g = f32dot(xs[...], gate_w[:, cols])
            u = f32dot(xs[...], up_w[:, cols])
            inner[:, cols] = (g / (1.0 + jnp.exp(-g)) * u).astype(BF16)
            return 0

        lax.fori_loop(0, 1024 // WIDE, first_half, 0)

        def second_half(q, _):
            cols = pl.ds(pl.multiple_of(q * CW, CW), CW)
            outs[q] = f32dot(inner[...], down_w[:, cols]).astype(BF16)
            return 0

        lax.fori_loop(0, 4, second_half, 0)
        osend[d] = f32dot(spread[...], outs[...].reshape(512, CW)).astype(BF16).reshape(32, 16, CW)

    def combine(d):
        p_wait(osend, oret, o_ss, o_rs, d)
        rows = oret[d].reshape(512, CW)
        part = f32dot(mix_hi[d], rows) + f32dot(mix_lo[d], rows)
        if d:
            ysend[d] = part.astype(BF16).reshape(4, 64, CW)
            z_copy(ysend, yback, y_ss, y_rs, d, -1).start()
        else:
            yback[0] = part.astype(BF16).reshape(4, 64, CW)

    dispatch(0, zsend)
    dispatch(1, zrecv)
    dispatch(3, zrecv)
    gate_load.wait()
    up_load.wait()
    down_load.wait()
    expert(0)
    dispatch(2, zrecv)
    for d in OFFSETS:
        expert(d)
        p_start(osend, oret, o_ss, o_rs, d)
    p_start(osend, oret, o_ss, o_rs, 0)
    for d in OFFSETS:
        combine(d)
    combine(0)
    for d in OFFSETS:
        z_copy(ysend, yback, y_ss, y_rs, d, -1).wait_recv()
    for q in range(4):
        cols = slice(q * CW, (q + 1) * CW)
        moe = f32dot(from_plane[...], jnp.concatenate([yback[d, q] for d in range(4)], axis=0))
        out_ref[:, cols] = (hidden_ref[:, cols].astype(F32) + moe).astype(BF16)

    for i in range(15):
        outgoing(i).wait_send()
    for d in range(1, 4):
        z_copy(msend, mrecv, m_ss, m_rs, d).wait_send()
        z_copy(zsend, zrecv, z_ss, z_rs, d).wait_send()
        z_copy(ysend, yback, y_ss, y_rs, d, -1).wait_send()

    def sent(i, _):
        for d in range(4):
            p_copy(psend, precv, p_ss, p_rs, i, d).wait_send()
            p_copy(osend, oret, o_ss, o_rs, i, d).wait_send()
        return 0

    lax.fori_loop(1, 32, sent, 0)


def layer(*arrays):
    vmem = pl.BlockSpec(memory_space=pltpu.VMEM)
    smem = pl.BlockSpec(memory_space=pltpu.SMEM)
    hbm = pl.BlockSpec(memory_space=pltpu.HBM)
    dma = pltpu.SemaphoreType.DMA
    return pl.pallas_call(
        layer_kernel,
        out_shape=pltpu.VMEM((128, 2048), BF16),
        in_specs=[hbm] * 3 + [vmem, smem, hbm, vmem, hbm, vmem, vmem, vmem] + [hbm] * 3,
        out_specs=vmem,
        scratch_shapes=[pltpu.VMEM((128, 1024), BF16)] * 3
        + [pltpu.VMEM((128, 2048), BF16), pltpu.VMEM((1024, 2048), BF16), pltpu.VMEM((128, 2048), BF16)]
        + [pltpu.VMEM((16, 208, 128), BF16)] * 2
        + [pltpu.VMEM((16, 64, 128), BF16)] * 2
        + [pltpu.VMEM((2048, 128), BF16)] * 3
        + [pltpu.VMEM((8, 2048), F32), pltpu.VMEM((128, 1024), BF16)]
        + [pltpu.VMEM((256, 128), BF16), pltpu.VMEM((128, 256), BF16), pltpu.VMEM((4, 512, 256), BF16)]
        + [pltpu.VMEM((4, 256, 512), BF16)] * 2
        + [pltpu.VMEM((512, 512), BF16)] * 2
        + [pltpu.VMEM((4, 64, 128), BF16)] * 2
        + [pltpu.VMEM((4, 4, 64, CW), BF16)] * 2
        + [pltpu.VMEM((4, 32, 16, CW), BF16)] * 4
        + [pltpu.VMEM((4, 4, 64, CW), BF16)] * 2
        + [pltpu.VMEM((2048, 1024), BF16)] * 2
        + [pltpu.VMEM((1024, 2048), BF16)]
        + [pltpu.VMEM((128, 2048), BF16), pltpu.VMEM((128, 1024), BF16), pltpu.VMEM((4, 128, CW), BF16)]
        + [dma((16,))] * 4
        + [dma((4,))] * 2
        + [dma((4,))] * 2
        + [dma((4, 32))] * 4
        + [dma((4,))] * 2
        + [dma((8,))],
        compiler_params=pltpu.CompilerParams(
            collective_id=1, has_side_effects=True, vmem_limit_bytes=60 * 2**20
        ),
    )(*arrays)


def on_device(
    stream,
    queries,
    keys_in,
    values_in,
    key_shift,
    head_shift,
    mix_gain,
    out_weight,
    post_gain,
    route,
    route_weight,
    w_gate,
    w_up,
    w_down,
):
    result = layer(
        queries[0], keys_in[0], values_in[0], key_shift[0].T, head_shift, stream[0], mix_gain[None],
        out_weight, post_gain[None], route[0].T, route_weight[0].T, w_gate[0], w_up[0], w_down[0],
    )
    return result[None]


def solution(mesh):
    placed = (
        P("dp", SP, None),
        P("dp", SP, None),
        P("dp", SP, None),
        P("dp", SP, None),
        P("dp", SP, None),
        P(),
        P(),
        P(),
        P(),
        P("dp", SP, None),
        P("dp", SP, None),
        P(SP_DP, None, None),
        P(SP_DP, None, None),
        P(SP_DP, None, None),
    )
    return jax.shard_map(
        on_device, mesh=mesh, in_specs=placed, out_specs=P("dp", SP, None), check_vma=False
    )
```
